256 devices in a mesh: sp: 32 (over z, y), tp: 8 (over x, core).
Axes of the slice: x: 4, y: 4, z: 8, core: 2. Of those that a mesh axis runs over, the one named last changes fastest.
Arguments:
- mixer_input: bfloat16 [4096, 1024], P('sp', 'tp'), may hold values from -1800 to 1800
- time_step: float32 [2, 64], P(None, 'tp'), may hold values from 0 to 2, as said below
- damping: float32 [2, 4096, 64], P(None, 'sp', 'tp'), may hold values from 0 to 2
- input_map: bfloat16 [2, 2, 64, 64, 16], P(None, None, 'tp'), may hold values from -1 to 1
- readout: float32 [2, 2, 64, 16, 64], P(None, None, 'tp'), may hold values from -0.5 to 0.5
- skip_gain: float32 [1024], P('tp'), may hold values from -4 to 4
- out_gain: float32 [1024], P('tp'), may hold values from 0.1 to 1.9
- out_weight: bfloat16 [1024, 2048], replicated, may hold values from -0.1875 to 0.1875
- residual: bfloat16 [4096, 2048], P(('sp', 'tp')), may hold values from -6 to 6
- channel_gain: float32 [2048], replicated, may hold values from 0.1 to 1.9
- value_weight: bfloat16 [2048, 6144], P('sp', 'tp'), may hold values from -0.125 to 0.125
- gate_weight: bfloat16 [2048, 6144], P('sp', 'tp'), may hold values from -0.125 to 0.125
- value_taps: float32 [3, 6144], P(None, 'tp'), may hold values from -3 to 3
- gate_taps: float32 [3, 6144], P(None, 'tp'), may hold values from -3 to 3
- down_weight: bfloat16 [6144, 2048], P('tp', 'sp'), may hold values from -0.078125 to 0.078125
Outputs:
- output: bfloat16 [4096, 2048], P(('sp', 'tp'))
The draws below stay inside these ranges and needn't reach their ends.
Inputs may be any that keep to these rules, and one draw needn't show every extreme that they name: `time_step`: positive.
All inputs are finite; a program needn't handle non-finite values.
Results may differ from the reference program's by a relative error of at most 0.017.
Values may be sent and summed in bfloat16 or wider, within the bound.
No kernel may reach another device: no remote copies, remote signals or barrier semaphores. Data moves between devices by JAX's collectives and lax.ppermute only.
A program may use at most 64 MiB of HBM per device.

```python
import math
import jax
import jax.numpy as jnp
from jax import lax

D = 2048
DS = 1024
GROUP = 16
STATE = 64
FF = 6144
TOK_DEV = 128
G = 64
TOKEN_POSITIONS = 4096
N_TP = 8


def draw_mixer_input(key, part):
    split_random_keys = jax.random.split(key, 3)
    column_pos = jnp.arange(DS, dtype=jnp.float32) / DS
    spread = math.log(10.0)
    noise = jnp.clip(jax.random.normal(split_random_keys[0], (TOKEN_POSITIONS, DS), jnp.float32), -5.0, 5.0)
    row_scale = jnp.exp(jax.random.uniform(split_random_keys[2], (TOKEN_POSITIONS, 1), jnp.float32, 0.0, spread))
    column_scale = jnp.exp(spread * column_pos)[None, :]
    return (noise * row_scale * column_scale).astype(jnp.float32).astype(jnp.bfloat16)


def draw_time_step(key, part):
    split_random_keys = jax.random.split(key, 3)
    group_count = DS // GROUP
    chance = jax.random.randint(split_random_keys[0], (2, group_count), 0, 16)
    quick = chance < 8
    quick_rate = jnp.exp(jax.random.uniform(split_random_keys[1], (2, group_count), jnp.float32, math.log(5.0 / TOK_DEV), math.log(16.0 / TOK_DEV)))
    slow_rate = jnp.exp(jax.random.uniform(split_random_keys[2], (2, group_count), jnp.float32, math.log(0.2 / TOKEN_POSITIONS), math.log(1.0 / TOKEN_POSITIONS)))
    return 2.0 * jnp.where(quick, quick_rate, slow_rate)


def draw_damping(key, part):
    split_random_keys = jax.random.split(key, 4)
    group_count = DS // GROUP
    blocks = TOKEN_POSITIONS // TOK_DEV
    baseline_rate = jnp.exp(jax.random.uniform(split_random_keys[0], (2, 1, group_count), jnp.float32, math.log(0.1), math.log(0.4))) / TOKEN_POSITIONS
    multiplier = jnp.exp(jax.random.uniform(split_random_keys[1], (2, blocks, group_count), jnp.float32, 0.0, math.log(4.0)))
    multiplier = jnp.repeat(multiplier, TOK_DEV, axis=1)
    spike_locations = jax.random.randint(split_random_keys[2], (2, 1, group_count, 3), 0, TOKEN_POSITIONS)
    dropped_fraction = jax.random.uniform(split_random_keys[3], (2, 1, group_count, 3), jnp.float32, 0.2, 0.33)
    token_position = jnp.arange(TOKEN_POSITIONS, dtype=jnp.int32)[None, :, None, None]
    sudden_spike = jnp.sum(jnp.where(token_position == spike_locations, -jnp.log1p(-dropped_fraction), 0.0), axis=3)
    return (baseline_rate * multiplier + sudden_spike).astype(jnp.float32)


def block_levels(rng, dims, cuts, smallest, top_value):
    level, own = 1.0, jax.random.fold_in(rng, 6)
    for axis_at, shards_of in cuts:
        draws = jnp.exp(jax.random.uniform(jax.random.fold_in(own, axis_at), (shards_of,), jnp.float32, smallest / len(cuts), top_value / len(cuts)))
        level = level * jnp.repeat(draws, dims[axis_at] // shards_of).reshape([-1 if axis == axis_at else 1 for axis in range(len(dims))])
    return level


def normal_values(rng, extent, scale, limit, cuts=(), kind=jnp.bfloat16):
    level = block_levels(rng, extent, cuts, -0.22, 0.18) if cuts else 1.0
    array = jax.random.normal(rng, extent, jnp.float32) * scale * level
    return jnp.minimum(jnp.maximum(array, -limit), limit).astype(kind)


def setup_inputs(seed: int = 0) -> dict:
    key_of = jax.random.split(jax.random.key(seed), 16)
    mixer_input = draw_mixer_input(jax.random.fold_in(key_of[15], 71), 0)
    time_step = draw_time_step(jax.random.fold_in(key_of[15], 71), 0)
    damping = draw_damping(jax.random.fold_in(key_of[15], 71), 0)
    input_map = normal_values(key_of[3], (2, 2, G, STATE, GROUP), (2 * GROUP) ** -0.5, 1.0, ((2, 8),))
    readout = normal_values(key_of[4], (2, 2, G, GROUP, STATE), (2 * STATE) ** -0.5, 0.5, ((2, 8),), jnp.float32)
    skip_gain = normal_values(key_of[5], (DS,), 1.0, 4.0, ((0, 8),), jnp.float32)
    out_gain = jnp.clip(1.0 + 0.18 * jax.random.normal(key_of[6], (DS,), jnp.float32), 0.1, 1.9)
    out_weight = normal_values(key_of[7], (DS, D), DS ** -0.5, 0.1875)
    residual = normal_values(key_of[8], (TOKEN_POSITIONS, D), 1.0, 6.0, ((0, 256),))
    channel_gain = jnp.clip(1.0 + 0.18 * jax.random.normal(key_of[9], (D,), jnp.float32), 0.1, 1.9)
    value_weight = normal_values(key_of[10], (D, FF), D ** -0.5, 0.125, ((0, 32), (1, 8)))
    gate_weight = normal_values(key_of[11], (D, FF), D ** -0.5, 0.125, ((0, 32), (1, 8)))
    value_taps = normal_values(key_of[12], (3, FF), 0.577, 3.0, ((1, 8),), jnp.float32)
    gate_taps = normal_values(key_of[13], (3, FF), 0.577, 3.0, ((1, 8),), jnp.float32)
    down_weight = normal_values(key_of[14], (FF, D), FF ** -0.5, 0.078125, ((0, 8), (1, 32)))
    return dict(mixer_input=mixer_input, time_step=time_step, damping=damping, input_map=input_map, readout=readout, skip_gain=skip_gain, out_gain=out_gain, out_weight=out_weight, residual=residual, channel_gain=channel_gain, value_weight=value_weight, gate_weight=gate_weight, value_taps=value_taps, gate_taps=gate_taps, down_weight=down_weight)


norm_eps = 1e-06
highest = lax.Precision.HIGHEST

def combine(earlier, latter):
    prod_real = latter[0] * earlier[0] - latter[1] * earlier[1]
    prod_imag = latter[0] * earlier[1] + latter[1] * earlier[0]
    sum_real = latter[0] * earlier[2] - latter[1] * earlier[3] + latter[2]
    sum_imag = latter[0] * earlier[3] + latter[1] * earlier[2] + latter[3]
    return (prod_real, prod_imag, sum_real, sum_imag)

def group_mixer(operands):
    group_input, step_pair, damp_pair, in_maps, out_maps = operands
    states = in_maps.shape[2]
    frequency = math.pi * jnp.arange(states, dtype=jnp.float32)
    result = jnp.zeros(group_input.shape, jnp.float32)
    for direction in range(2):
        step_size = step_pair[direction]
        rotation = step_size * frequency
        magnitude = jnp.exp(-0.5 * step_size - damp_pair[direction])[:, None]
        decay_real = magnitude * jnp.cos(rotation)[None, :]
        decay_imag = magnitude * jnp.sin(rotation)[None, :]
        in_scale = jnp.sqrt(-jnp.expm1(-step_size))
        drive_real = jnp.dot(group_input, in_maps[direction, 0].T, preferred_element_type=jnp.float32) * in_scale
        drive_imag = jnp.dot(group_input, in_maps[direction, 1].T, preferred_element_type=jnp.float32) * in_scale
        scanned = lax.associative_scan(combine, (decay_real, decay_imag, drive_real, drive_imag), reverse=direction == 1, axis=0)
        result = result + jnp.dot(scanned[2], out_maps[direction, 0].T, precision=highest)
        result = result - jnp.dot(scanned[3], out_maps[direction, 1].T, precision=highest)
    return result

def shifted_sum(values, tap_rows):
    widened = jnp.pad(values.astype(jnp.float32), ((1, 1), (0, 0)))
    return tap_rows[0] * widened[:-2] + tap_rows[1] * widened[1:-1] + tap_rows[2] * widened[2:]

def reference(mixer_input, time_step, damping, input_map, readout, skip_gain, out_gain, out_weight, residual, channel_gain, value_weight, gate_weight, value_taps, gate_taps, down_weight):
    tokens, channels = mixer_input.shape
    group_count = time_step.shape[1]
    group_width = channels // group_count
    grouped = jnp.transpose(mixer_input.reshape(tokens, group_count, group_width), (1, 0, 2))
    per_group = lax.map(group_mixer, (grouped, time_step.T, jnp.transpose(damping, (2, 0, 1)), jnp.moveaxis(input_map, 2, 0), jnp.moveaxis(readout, 2, 0)))
    mixed_y = jnp.transpose(per_group, (1, 0, 2)).reshape(tokens, channels) + skip_gain[None, :] * mixer_input.astype(jnp.float32)
    inverse = lax.rsqrt(lax.optimization_barrier(jnp.mean(mixed_y * mixed_y, axis=1, keepdims=True)) + norm_eps)
    normed_mix = (mixed_y * inverse * out_gain[None, :]).astype(jnp.bfloat16)
    mixed_rows = jnp.dot(normed_mix, out_weight, preferred_element_type=jnp.float32)
    hidden_state = (residual.astype(jnp.float32) + mixed_rows).astype(jnp.bfloat16)
    state_wide = hidden_state.astype(jnp.float32)
    scale_rows = lax.rsqrt(lax.optimization_barrier(jnp.mean(state_wide * state_wide, axis=1, keepdims=True)) + norm_eps)
    normed = (state_wide * scale_rows * channel_gain[None, :]).astype(jnp.bfloat16)
    value_up = jnp.dot(normed, value_weight, preferred_element_type=jnp.float32).astype(jnp.bfloat16)
    gate_up = jnp.dot(normed, gate_weight, preferred_element_type=jnp.float32).astype(jnp.bfloat16)
    value_conv = shifted_sum(value_up, value_taps)
    gate_conv = shifted_sum(gate_up, gate_taps)
    hidden = (value_conv * jax.nn.silu(gate_conv)).astype(jnp.bfloat16)
    block_width = FF // N_TP
    summed = jnp.zeros((tokens, out_weight.shape[1]), jnp.float32)
    for part_index in range(N_TP):
        first_col = part_index * block_width
        partial_value = jnp.dot(hidden[:, first_col:first_col + block_width], down_weight[first_col:first_col + block_width], preferred_element_type=jnp.float32)
        rounded = lax.optimization_barrier(partial_value.astype(jnp.bfloat16))
        summed = summed + rounded.astype(jnp.float32)
    return (state_wide + summed).astype(jnp.bfloat16)
```

```python
import math

import jax
import jax.numpy as jnp
from jax import lax
from jax.experimental import pallas as pl
from jax.experimental.pallas import tpu as pltpu
from jax.sharding import Mesh
from jax.sharding import PartitionSpec as P


norm_eps = 1e-06
SP = ("z", "yh", "yl")
TP = ("x", "c")
VMEM = pl.BlockSpec(memory_space=pltpu.VMEM)
SMEM = pl.BlockSpec(memory_space=pltpu.SMEM)


def shifted(array, axis, step):
    n = lax.axis_size(axis)
    return lax.ppermute(array, axis, [(i, (i + step) % n) for i in range(n)])


def sent_to_all(array, axis):
    copies = jnp.broadcast_to(array, (lax.axis_size(axis), *array.shape))
    return lax.all_to_all(copies, axis, split_axis=0, concat_axis=0, tiled=True)


def step_decays(table, damp_ref):
    rows = damp_ref.shape[2]
    half = damp_ref.shape[1], rows
    fwd = jnp.exp(-jnp.broadcast_to(table[3][:, :1], half) - damp_ref[0])
    bwd = jnp.exp(-jnp.broadcast_to(table[3][:, 64:65], half) - damp_ref[1])
    return fwd, bwd


def local_kernel(x_ref, table_ref, damp_ref, map_ref, end_ref, dre_ref, dim_ref):
    rows = x_ref.shape[0]
    groups = map_ref.shape[2]
    width = map_ref.shape[3]
    x = x_ref[...]
    scale = table_ref[2]
    owner = lax.broadcasted_iota(jnp.int32, (groups * width, 256), 0) // width
    for g in range(groups):
        block = jnp.concatenate(
            [map_ref[0, 0, g], map_ref[1, 0, g], map_ref[0, 1, g], map_ref[1, 1, g]], axis=1
        ).astype(jnp.float32)
        block = jnp.concatenate([block] * groups, axis=0)
        block = jnp.where(owner == g, block, 0.0).astype(jnp.bfloat16)
        drive = jnp.dot(x, block, preferred_element_type=jnp.float32)
        dre_ref[:, g, :] = drive[:, :128] * scale[g : g + 1, :]
        dim_ref[:, g, :] = drive[:, 128:] * scale[g : g + 1, :]
    cos, sin = table_ref[0], table_ref[1]
    lane_fwd = lax.broadcasted_iota(jnp.int32, (groups, 128), 1) < 64
    fwd, bwd = step_decays(table_ref, damp_ref)
    real = jnp.zeros((groups, 128), jnp.float32)
    imag = jnp.zeros((groups, 128), jnp.float32)
    for i in range(rows):
        j = rows - 1 - i
        size = jnp.where(
            lane_fwd,
            jnp.broadcast_to(fwd[:, i : i + 1], (groups, 128)),
            jnp.broadcast_to(bwd[:, j : j + 1], (groups, 128)),
        )
        dec_re, dec_im = size * cos, size * sin
        drive_re = jnp.where(lane_fwd, dre_ref[i], dre_ref[j])
        drive_im = jnp.where(lane_fwd, dim_ref[i], dim_ref[j])
        real, imag = (
            dec_re * real - dec_im * imag + drive_re,
            dec_re * imag + dec_im * real + drive_im,
        )
    total = jnp.sum(damp_ref[...], axis=2, keepdims=True)
    total = jnp.where(
        lane_fwd,
        jnp.broadcast_to(total[0], (groups, 128)),
        jnp.broadcast_to(total[1], (groups, 128)),
    )
    end_ref[:, :128] = real
    end_ref[:, 128:256] = imag
    end_ref[:, 256:] = total + rows * table_ref[3]


def mix_kernel(
    at_ref,
    ends_ref,
    dre_ref,
    dim_ref,
    table_ref,
    damp_ref,
    read_ref,
    x_ref,
    skip_ref,
    gain_ref,
    out_ref,
    fre_ref,
    fim_ref,
    bre_ref,
    bim_ref,
):
    rows = x_ref.shape[0]
    groups = dre_ref.shape[1]
    blocks = ends_ref.shape[0]
    at = at_ref[0]
    cos, sin = table_ref[0], table_ref[1]
    lane_fwd = lax.broadcasted_iota(jnp.int32, (groups, 128), 1) < 64
    block_re, block_im = cos, sin
    power = 1
    while power < rows:
        block_re, block_im = block_re * block_re - block_im * block_im, 2.0 * block_re * block_im
        power *= 2
    real = jnp.zeros((groups, 128), jnp.float32)
    imag = jnp.zeros((groups, 128), jnp.float32)
    for i in range(blocks):
        j = blocks - 1 - i
        part = jnp.where(lane_fwd, ends_ref[i, :, 256:], ends_ref[j, :, 256:])
        size = jnp.exp(-part)
        dec_re, dec_im = size * block_re, size * block_im
        end_re = jnp.where(lane_fwd, ends_ref[i, :, :128], ends_ref[j, :, :128])
        end_im = jnp.where(lane_fwd, ends_ref[i, :, 128:256], ends_ref[j, :, 128:256])
        next_re = dec_re * real - dec_im * imag + end_re
        next_im = dec_re * imag + dec_im * real + end_im
        keep_fwd = jnp.where(i < at, 1, 0)
        keep_bwd = jnp.where(j > at, 1, 0)
        keep = jnp.where(lane_fwd, keep_fwd, keep_bwd) == 1
        real = jnp.where(keep, next_re, real)
        imag = jnp.where(keep, next_im, imag)
    fwd, bwd = step_decays(table_ref, damp_ref)
    for i in range(rows):
        j = rows - 1 - i
        size = jnp.where(
            lane_fwd,
            jnp.broadcast_to(fwd[:, i : i + 1], (groups, 128)),
            jnp.broadcast_to(bwd[:, j : j + 1], (groups, 128)),
        )
        dec_re, dec_im = size * cos, size * sin
        drive_re = jnp.where(lane_fwd, dre_ref[i], dre_ref[j])
        drive_im = jnp.where(lane_fwd, dim_ref[i], dim_ref[j])
        real, imag = (
            dec_re * real - dec_im * imag + drive_re,
            dec_re * imag + dec_im * real + drive_im,
        )
        fre_ref[i] = real
        fim_ref[i] = imag
        bre_ref[j] = real
        bim_ref[j] = imag
    width = read_ref.shape[3]
    channels = groups * width
    table = jnp.concatenate(
        [
            read_ref[0, 0].reshape(channels, 64),
            read_ref[1, 0].reshape(channels, 64),
            -read_ref[0, 1].reshape(channels, 64),
            -read_ref[1, 1].reshape(channels, 64),
        ],
        axis=1,
    )
    owner = lax.broadcasted_iota(jnp.int32, (channels, 256), 0) // width
    row_fwd = lax.broadcasted_iota(jnp.int32, (rows, 128), 1) < 64
    mixed = skip_ref[...] * x_ref[...].astype(jnp.float32)
    for g in range(groups):
        state = jnp.concatenate(
            [
                jnp.where(row_fwd, fre_ref[:, g, :], bre_ref[:, g, :]),
                jnp.where(row_fwd, fim_ref[:, g, :], bim_ref[:, g, :]),
            ],
            axis=1,
        ).astype(jnp.bfloat16)
        part = jnp.where(owner == g, table, 0.0).astype(jnp.bfloat16)
        mixed = mixed + lax.dot_general(
            state, part, (((1,), (1,)), ((), ())), preferred_element_type=jnp.float32
        )
    parts = out_ref.shape[0]
    own = rows // parts
    for p in range(parts):
        out_ref[p, :own, :] = mixed[p * own : (p + 1) * own, :]
        out_ref[p, own:, :] = jnp.broadcast_to(gain_ref[...], (8, channels))


def mixer_branch(mixer_input, time_step, damping, input_map, readout, skip_gain, out_gain):
    rows = mixer_input.shape[0]
    groups = time_step.shape[1]
    states = input_map.shape[3]
    frequency = math.pi * jnp.arange(states, dtype=jnp.float32)
    step = time_step.T[:, :, None]
    shape = (groups, 2, states)
    rotation = step * frequency
    table = jnp.stack(
        [
            jnp.cos(rotation),
            jnp.sin(rotation),
            jnp.broadcast_to(jnp.sqrt(-jnp.expm1(-step)), shape),
            jnp.broadcast_to(0.5 * step, shape),
        ]
    ).reshape(4, groups, 2 * states)
    damp = jnp.swapaxes(damping, 1, 2)
    maps = jnp.swapaxes(input_map, 3, 4)
    drive_shape = jax.ShapeDtypeStruct((rows, groups, 2 * states), jnp.float32)
    ends, drive_re, drive_im = pl.pallas_call(
        local_kernel,
        out_shape=(
            jax.ShapeDtypeStruct((groups, 6 * states), jnp.float32),
            drive_shape,
            drive_shape,
        ),
        in_specs=[VMEM] * 4,
        out_specs=(VMEM,) * 3,
        name="mixer_local",
        cost_estimate=pl.CostEstimate(
            flops=300_000_000, bytes_accessed=2_000_000, transcendentals=0
        ),
    )(mixer_input, table, damp, maps)
    all_ends = sent_to_all(ends, SP)
    at = lax.axis_index(SP).astype(jnp.int32).reshape(1)
    scratch = pltpu.VMEM((rows, groups, 2 * states), jnp.float32)
    parts = lax.axis_size(TP)
    return pl.pallas_call(
        mix_kernel,
        out_shape=jax.ShapeDtypeStruct(
            (parts, rows // parts + 8, mixer_input.shape[1]), jnp.float32
        ),
        in_specs=[SMEM] + [VMEM] * 9,
        out_specs=VMEM,
        scratch_shapes=[scratch] * 4,
        name="mixer_out",
        cost_estimate=pl.CostEstimate(
            flops=300_000_000, bytes_accessed=2_000_000, transcendentals=0
        ),
    )(
        at,
        all_ends,
        drive_re,
        drive_im,
        table,
        damp,
        readout,
        mixer_input,
        skip_gain[None, :],
        out_gain[None, :],
    )


def z_ring(block):
    found = {0: block}
    up = down = block
    for s in range(1, 4):
        up = shifted(up, "z", 1)
        down = shifted(down, "z", -1)
        found[8 - s], found[s] = up, down
    half = block.shape[0] // 2
    far_up = shifted(up[:half], "z", 1)
    found[4] = (far_up, shifted(down[half:], "z", -1))
    return found


def edge_rows(cells):
    last = cells.shape[1] - 1
    edges = jnp.concatenate((cells[0, :1], cells[0, last:], cells[1, :1], cells[1, last:]))
    near = lax.ppermute(edges, "yl", [(0, 1), (1, 0)])
    count = lax.axis_size("z")
    pairs = [(2 * i + 1, 2 * i + 2) for i in range(count - 1)]
    far = lax.ppermute(
        jnp.where(lax.axis_index("yl") == 0, edges[:1], edges[3:]),
        ("z", "yl"),
        pairs + [(j, i) for i, j in pairs],
    )
    return near, far


def ffn_kernel(at_ref, cells_ref, near_ref, far_ref, vtap_ref, gtap_ref, *refs):
    line = refs[:9]
    out_ref, whole_ref, rows_ref = refs[9:]
    z, low = at_ref[0], at_ref[1]
    tok = cells_ref.shape[1]
    total = tok + 16
    width = vtap_ref.shape[1]
    cut = line[0].shape[0]
    for ref in range(9):
        size = line[ref].shape[0]
        start = lax.rem(z + (ref if ref < 5 else ref - 1), 8) * cut
        if ref == 5:
            start = start + cut // 2
        whole_ref[pl.ds(pl.multiple_of(start, cut // 2), size), :] = line[ref][...]
    row = lax.broadcasted_iota(jnp.int32, (16, cells_ref.shape[2]), 0)
    even = jnp.full(row.shape, low, jnp.int32) == 0
    near = [
        jnp.broadcast_to(near_ref[k : k + 1, :].astype(jnp.float32), row.shape) for k in range(4)
    ]
    far = jnp.broadcast_to(far_ref[...].astype(jnp.float32), row.shape)
    sides = (
        (jnp.where(even, near[0], near[2]), jnp.where(even, far, near[1])),
        (jnp.where(even, near[2], far), jnp.where(even, near[1], near[3])),
    )
    for k in range(2):
        after, before = sides[k]
        tile = jnp.where(row == 0, after, jnp.where(row == 1, before, 0.0))
        rows_ref[k * total : k * total + tok, :] = cells_ref[k]
        rows_ref[k * total + tok : (k + 1) * total, :] = tile.astype(jnp.bfloat16)
    both = jnp.dot(
        rows_ref[...], whole_ref[:, : 2 * width], preferred_element_type=jnp.float32
    )
    both = both.astype(jnp.bfloat16).astype(jnp.float32)

    def convolved(up, taps):
        mid, after, before = up[:tok], up[tok : tok + 1], up[tok + 1 : tok + 2]
        at = lax.broadcasted_iota(jnp.int32, mid.shape, 0)
        prev = jnp.where(at == 0, jnp.broadcast_to(before, mid.shape), pltpu.roll(mid, 1, 0))
        foll = jnp.where(
            at == tok - 1, jnp.broadcast_to(after, mid.shape), pltpu.roll(mid, tok - 1, 0)
        )
        return taps[0:1] * prev + taps[1:2] * mid + taps[2:3] * foll

    hidden = []
    for k in range(2):
        part = both[k * total : (k + 1) * total]
        value = convolved(part[:, :width], vtap_ref[...])
        gate = convolved(part[:, width:], gtap_ref[...])
        hidden.append((value * (gate / (1.0 + jnp.exp(-gate)))).astype(jnp.bfloat16))
    sums = lax.dot_general(
        jnp.concatenate(hidden, axis=0),
        whole_ref[:, 2 * width :],
        (((1,), (1,)), ((), ())),
        preferred_element_type=jnp.float32,
    ).astype(jnp.bfloat16)
    own = out_ref.shape[1]
    for p in range(out_ref.shape[0]):
        out_ref[p] = sums[p * own : (p + 1) * own]


def body(
    mixer_input,
    time_step,
    damping,
    input_map,
    readout,
    skip_gain,
    out_gain,
    out_weight,
    residual,
    channel_gain,
    value_weight,
    gate_weight,
    value_taps,
    gate_taps,
    down_weight,
):
    half = value_weight.shape[1] // 2
    halves = [
        jnp.concatenate((value_weight[:, cut], gate_weight[:, cut], down_weight.T[:, cut]), axis=1)
        for cut in (slice(0, half), slice(half, 2 * half))
    ]
    crossed = lax.all_to_all(
        jnp.stack((halves[0], halves[0], halves[1], halves[1])), ("yh", "yl"), 0, 0, tiled=True
    )
    pieces = z_ring(crossed.reshape(-1, 3 * half))
    mixed_y = mixer_branch(
        mixer_input, time_step, damping, input_map, readout, skip_gain, out_gain
    )
    tok_rows, local_width = mixer_input.shape
    tp_count = lax.axis_size(TP)
    own_rows = tok_rows // tp_count
    arrived = lax.all_to_all(mixed_y, TP, 0, 0, tiled=True)
    gains = arrived[:, own_rows].reshape(tp_count * local_width)
    rows_y = jnp.moveaxis(arrived[:, :own_rows], 0, 1).reshape(own_rows, tp_count * local_width)
    inverse = lax.rsqrt(jnp.mean(rows_y * rows_y, axis=1, keepdims=True) + norm_eps)
    token_block = (rows_y * inverse * gains[None, :]).astype(jnp.bfloat16)
    mixed_rows = jnp.dot(token_block, out_weight, preferred_element_type=jnp.float32)
    hidden_state = (residual.astype(jnp.float32) + mixed_rows).astype(jnp.bfloat16)
    state_wide = hidden_state.astype(jnp.float32)
    scale_rows = lax.rsqrt(jnp.mean(state_wide * state_wide, axis=1, keepdims=True) + norm_eps)
    normed = (state_wide * scale_rows * channel_gain[None, :]).astype(jnp.bfloat16)
    model = normed.shape[1]
    cells = sent_to_all(normed, ("yh", *TP)).reshape(2, tok_rows, model)
    near, far = edge_rows(cells)
    place = jnp.stack([lax.axis_index("z"), lax.axis_index("yl")]).astype(jnp.int32)
    shift = lax.axis_index("yh") * half
    taps = [lax.dynamic_slice(t, (0, shift), (3, half)) for t in (value_taps, gate_taps)]
    ordered = [*(pieces[d] for d in range(4)), *pieces[4], *(pieces[d] for d in range(5, 8))]
    partial = pl.pallas_call(
        ffn_kernel,
        out_shape=jax.ShapeDtypeStruct((2 * tp_count, own_rows, model), jnp.bfloat16),
        in_specs=[SMEM] + [VMEM] * (5 + len(ordered)),
        out_specs=VMEM,
        scratch_shapes=[
            pltpu.VMEM((model, 3 * half), jnp.bfloat16),
            pltpu.VMEM((2 * (tok_rows + 16), model), jnp.bfloat16),
        ],
        name="ffn",
        cost_estimate=pl.CostEstimate(
            flops=1_300_000_000, bytes_accessed=6_000_000, transcendentals=100_000
        ),
    )(place, cells, near, far, *taps, *ordered)
    parts = lax.all_to_all(partial, ("yh", *TP), 0, 0, tiled=True)
    summed = parts.astype(jnp.float32).sum(axis=0)
    return (state_wide + summed).astype(jnp.bfloat16)


def solution(mesh):
    fine = Mesh(mesh.devices.reshape(8, 2, 2, 4, 2), ("z", "yh", "yl", "x", "c"))
    in_specs = (
        P(SP, TP),
        P(None, TP),
        P(None, SP, TP),
        P(None, None, TP, None, None),
        P(None, None, TP, None, None),
        P(TP),
        P(TP),
        P(),
        P((*SP, *TP), None),
        P(),
        P(SP, TP),
        P(SP, TP),
        P(None, TP),
        P(None, TP),
        P(TP, SP),
    )
    out_specs = P((*SP, *TP), None)

    return jax.shard_map(body, mesh=fine, in_specs=in_specs, out_specs=out_specs, check_vma=False)
```

```python
import math

import jax
import jax.numpy as jnp
from jax import lax
from jax.experimental import pallas as pl
from jax.experimental.pallas import tpu as pltpu
from jax.sharding import Mesh
from jax.sharding import PartitionSpec as P


norm_eps = 1e-06
SP = ("z", "yh", "yl")
TP = ("x", "c")
PAIR = ("yl", "x", "c")
VMEM = pl.BlockSpec(memory_space=pltpu.VMEM)
SMEM = pl.BlockSpec(memory_space=pltpu.SMEM)


def shifted(array, axis, step):
    n = lax.axis_size(axis)
    return lax.ppermute(array, axis, [(i, (i + step) % n) for i in range(n)])


def step_decays(table, damp_ref):
    rows = damp_ref.shape[2]
    half = damp_ref.shape[1], rows
    fwd = jnp.exp(-jnp.broadcast_to(table[3][:, :1], half) - damp_ref[0])
    bwd = jnp.exp(-jnp.broadcast_to(table[3][:, 64:65], half) - damp_ref[1])
    return fwd, bwd


def local_kernel(x_ref, table_ref, damp_ref, map_ref, end_ref, dre_ref, dim_ref):
    rows = x_ref.shape[0]
    groups = map_ref.shape[2]
    width = map_ref.shape[3]
    x = x_ref[...]
    scale = table_ref[2]
    owner = lax.broadcasted_iota(jnp.int32, (groups * width, 256), 0) // width
    for g in range(groups):
        block = jnp.concatenate(
            [map_ref[0, 0, g], map_ref[1, 0, g], map_ref[0, 1, g], map_ref[1, 1, g]], axis=1
        ).astype(jnp.float32)
        block = jnp.concatenate([block] * groups, axis=0)
        block = jnp.where(owner == g, block, 0.0).astype(jnp.bfloat16)
        drive = jnp.dot(x, block, preferred_element_type=jnp.float32)
        dre_ref[:, g, :] = drive[:, :128] * scale[g : g + 1, :]
        dim_ref[:, g, :] = drive[:, 128:] * scale[g : g + 1, :]
    cos, sin = table_ref[0], table_ref[1]
    lane_fwd = lax.broadcasted_iota(jnp.int32, (groups, 128), 1) < 64
    fwd, bwd = step_decays(table_ref, damp_ref)
    real = jnp.zeros((groups, 128), jnp.float32)
    imag = jnp.zeros((groups, 128), jnp.float32)
    for i in range(rows):
        j = rows - 1 - i
        size = jnp.where(
            lane_fwd,
            jnp.broadcast_to(fwd[:, i : i + 1], (groups, 128)),
            jnp.broadcast_to(bwd[:, j : j + 1], (groups, 128)),
        )
        dec_re, dec_im = size * cos, size * sin
        drive_re = jnp.where(lane_fwd, dre_ref[i], dre_ref[j])
        drive_im = jnp.where(lane_fwd, dim_ref[i], dim_ref[j])
        real, imag = (
            dec_re * real - dec_im * imag + drive_re,
            dec_re * imag + dec_im * real + drive_im,
        )
    total = jnp.sum(damp_ref[...], axis=2, keepdims=True)
    total = jnp.where(
        lane_fwd,
        jnp.broadcast_to(total[0], (groups, 128)),
        jnp.broadcast_to(total[1], (groups, 128)),
    )
    total = total + rows * table_ref[3]
    high = total.astype(jnp.bfloat16)
    low = (total - high.astype(jnp.float32)).astype(jnp.bfloat16).astype(jnp.float32)
    lane = lax.broadcasted_iota(jnp.int32, (groups, 128), 1)
    total = jnp.where(lane % 64 < 32, high.astype(jnp.float32), low).astype(jnp.bfloat16)
    real, imag = real.astype(jnp.bfloat16), imag.astype(jnp.bfloat16)
    for p in range(end_ref.shape[0]):
        end_ref[p, :, :128] = real
        end_ref[p, :, 128:256] = imag
        end_ref[p, :, 256:] = total


def mix_kernel(
    at_ref,
    ends_ref,
    dre_ref,
    dim_ref,
    table_ref,
    damp_ref,
    read_ref,
    x_ref,
    skip_ref,
    gain_ref,
    out_ref,
    fre_ref,
    fim_ref,
    bre_ref,
    bim_ref,
):
    rows = x_ref.shape[0]
    groups = dre_ref.shape[1]
    blocks = ends_ref.shape[0]
    at = at_ref[0]
    cos, sin = table_ref[0], table_ref[1]
    lane_fwd = lax.broadcasted_iota(jnp.int32, (groups, 128), 1) < 64
    block_re, block_im = cos, sin
    power = 1
    while power < rows:
        block_re, block_im = block_re * block_re - block_im * block_im, 2.0 * block_re * block_im
        power *= 2
    lane_high = lax.broadcasted_iota(jnp.int32, (groups, 128), 1) % 64 < 32

    def picked(i, j, at):
        fwd_part = ends_ref[i, :, at : at + 128].astype(jnp.float32)
        return jnp.where(lane_fwd, fwd_part, ends_ref[j, :, at : at + 128].astype(jnp.float32))

    real = jnp.zeros((groups, 128), jnp.float32)
    imag = jnp.zeros((groups, 128), jnp.float32)
    for i in range(blocks):
        j = blocks - 1 - i
        part = picked(i, j, 256)
        part = part + jnp.where(lane_high, pltpu.roll(part, 96, 1), pltpu.roll(part, 32, 1))
        size = jnp.exp(-part)
        dec_re, dec_im = size * block_re, size * block_im
        end_re, end_im = picked(i, j, 0), picked(i, j, 128)
        next_re = dec_re * real - dec_im * imag + end_re
        next_im = dec_re * imag + dec_im * real + end_im
        keep_fwd = jnp.where(i < at, 1, 0)
        keep_bwd = jnp.where(j > at, 1, 0)
        keep = jnp.where(lane_fwd, keep_fwd, keep_bwd) == 1
        real = jnp.where(keep, next_re, real)
        imag = jnp.where(keep, next_im, imag)
    fwd, bwd = step_decays(table_ref, damp_ref)
    for i in range(rows):
        j = rows - 1 - i
        size = jnp.where(
            lane_fwd,
            jnp.broadcast_to(fwd[:, i : i + 1], (groups, 128)),
            jnp.broadcast_to(bwd[:, j : j + 1], (groups, 128)),
        )
        dec_re, dec_im = size * cos, size * sin
        drive_re = jnp.where(lane_fwd, dre_ref[i], dre_ref[j])
        drive_im = jnp.where(lane_fwd, dim_ref[i], dim_ref[j])
        real, imag = (
            dec_re * real - dec_im * imag + drive_re,
            dec_re * imag + dec_im * real + drive_im,
        )
        fre_ref[i] = real
        fim_ref[i] = imag
        bre_ref[j] = real
        bim_ref[j] = imag
    width = read_ref.shape[3]
    channels = groups * width
    table = jnp.concatenate(
        [
            read_ref[0, 0].reshape(channels, 64),
            read_ref[1, 0].reshape(channels, 64),
            -read_ref[0, 1].reshape(channels, 64),
            -read_ref[1, 1].reshape(channels, 64),
        ],
        axis=1,
    )
    owner = lax.broadcasted_iota(jnp.int32, (channels, 256), 0) // width
    row_fwd = lax.broadcasted_iota(jnp.int32, (rows, 128), 1) < 64
    mixed = skip_ref[...] * x_ref[...].astype(jnp.float32)
    for g in range(groups):
        state = jnp.concatenate(
            [
                jnp.where(row_fwd, fre_ref[:, g, :], bre_ref[:, g, :]),
                jnp.where(row_fwd, fim_ref[:, g, :], bim_ref[:, g, :]),
            ],
            axis=1,
        ).astype(jnp.bfloat16)
        part = jnp.where(owner == g, table, 0.0).astype(jnp.bfloat16)
        mixed = mixed + lax.dot_general(
            state, part, (((1,), (1,)), ((), ())), preferred_element_type=jnp.float32
        )
    high = gain_ref[...].astype(jnp.bfloat16).astype(jnp.float32)
    mid = (gain_ref[...] - high).astype(jnp.bfloat16).astype(jnp.float32)
    low = gain_ref[...] - high - mid
    row = lax.broadcasted_iota(jnp.int32, (16, channels), 0)
    tail = jnp.zeros(row.shape, jnp.float32)
    for k, part in enumerate((high, mid, low)):
        tail = jnp.where(row == k, jnp.broadcast_to(part, row.shape), tail)
    mixed, tail = mixed.astype(jnp.bfloat16), tail.astype(jnp.bfloat16)
    for p in range(out_ref.shape[0]):
        out_ref[p, :rows, :] = mixed
        out_ref[p, rows:, :] = tail


def mixer_branch(mixer_input, time_step, damping, input_map, readout, skip_gain, out_gain):
    rows = mixer_input.shape[0]
    groups = time_step.shape[1]
    states = input_map.shape[3]
    frequency = math.pi * jnp.arange(states, dtype=jnp.float32)
    step = time_step.T[:, :, None]
    shape = (groups, 2, states)
    rotation = step * frequency
    table = jnp.stack(
        [
            jnp.cos(rotation),
            jnp.sin(rotation),
            jnp.broadcast_to(jnp.sqrt(-jnp.expm1(-step)), shape),
            jnp.broadcast_to(0.5 * step, shape),
        ]
    ).reshape(4, groups, 2 * states)
    damp = jnp.swapaxes(damping, 1, 2)
    maps = jnp.swapaxes(input_map, 3, 4)
    drive_shape = jax.ShapeDtypeStruct((rows, groups, 2 * states), jnp.float32)
    ends, drive_re, drive_im = pl.pallas_call(
        local_kernel,
        out_shape=(
            jax.ShapeDtypeStruct((lax.axis_size(SP), groups, 6 * states), jnp.bfloat16),
            drive_shape,
            drive_shape,
        ),
        in_specs=[VMEM] * 4,
        out_specs=(VMEM,) * 3,
        name="mixer_local",
        cost_estimate=pl.CostEstimate(
            flops=300_000_000, bytes_accessed=2_000_000, transcendentals=0
        ),
    )(mixer_input, table, damp, maps)
    all_ends = lax.all_to_all(ends, SP, 0, 0, tiled=True)
    at = lax.axis_index(SP).astype(jnp.int32).reshape(1)
    scratch = pltpu.VMEM((rows, groups, 2 * states), jnp.float32)
    copies = lax.axis_size(PAIR)
    return pl.pallas_call(
        mix_kernel,
        out_shape=jax.ShapeDtypeStruct(
            (copies, rows + 16, mixer_input.shape[1]), jnp.bfloat16
        ),
        in_specs=[SMEM] + [VMEM] * 9,
        out_specs=VMEM,
        scratch_shapes=[scratch] * 4,
        name="mixer_out",
        cost_estimate=pl.CostEstimate(
            flops=300_000_000, bytes_accessed=2_000_000, transcendentals=0
        ),
    )(
        at,
        all_ends,
        drive_re,
        drive_im,
        table,
        damp,
        readout,
        mixer_input,
        skip_gain[None, :],
        out_gain[None, :],
    )


def z_ring(block):
    found = {0: block}
    up = down = block
    for s in range(1, 5):
        found[8 - s] = up = shifted(up, "z", 1)
        if s < 4:
            found[s] = down = shifted(down, "z", -1)
    return [found[d] for d in range(8)]


def pair_rows(rows):
    both = jnp.stack((rows, lax.ppermute(rows, "yl", [(0, 1), (1, 0)])))
    quad = jnp.concatenate((both, lax.ppermute(both, "c", [(0, 1), (1, 0)])))
    pieces = {0: quad}
    for d in (1, 3, 2):
        pieces[d] = shifted(quad, "x", -d)
    return [pieces[d] for d in range(4)]


def edges_passed(near, far):
    pairs = [(2 * i + 1, 2 * i + 2) for i in range(lax.axis_size("z") - 1)]
    far = lax.ppermute(far, ("z", "yh"), pairs + [(j, i) for i, j in pairs])
    near = lax.ppermute(near, "yh", [(0, 1), (1, 0)])
    return near, far


def pack_kernel(value_ref, gate_ref, down_ref, out_ref):
    half = value_ref.shape[1] // 2
    for k in range(out_ref.shape[0]):
        cut = slice(k % 2 * half, (k % 2 + 1) * half)
        out_ref[k, :, :half] = value_ref[:, cut]
        out_ref[k, :, half : 2 * half] = gate_ref[:, cut]
        out_ref[k, :, 2 * half :] = down_ref[:, cut]


def pair_gains(mixed_ref, tok):
    parts = [mixed_ref[p, tok:, :].astype(jnp.float32) for p in range(mixed_ref.shape[0] // 2)]
    return jnp.concatenate([g[0:1] + g[1:2] + g[2:3] for g in parts], axis=1)


def pair_residual(at_ref, pieces, state_ref):
    low, x, core = at_ref[0], at_ref[1], at_ref[2]
    own = pieces[0].shape[1]
    for dx, ref in enumerate(pieces):
        for k in range(4):
            row = lax.rem(low + k % 2, 2) * 8 + lax.rem(x + dx, 4) * 2 + lax.rem(core + k // 2, 2)
            state_ref[pl.ds(pl.multiple_of(row * own, own), own), :] = ref[k]


def normed_rows(mixed, resid, gains, weight, gain):
    mixed = mixed.astype(jnp.float32)
    inverse = lax.rsqrt(jnp.mean(mixed * mixed, axis=1, keepdims=True) + norm_eps)
    normed_mix = (mixed * inverse * gains).astype(jnp.bfloat16)
    added = jnp.dot(normed_mix, weight, preferred_element_type=jnp.float32)
    state = (resid.astype(jnp.float32) + added).astype(jnp.bfloat16)
    wide = state.astype(jnp.float32)
    scale = lax.rsqrt(jnp.mean(wide * wide, axis=1, keepdims=True) + norm_eps)
    return state, (wide * scale * gain).astype(jnp.bfloat16)


def edge_kernel(at_ref, mixed_ref, weight_ref, gain_ref, r0, r1, r2, r3, *refs):
    near_ref, far_ref, state_ref = refs
    tok = mixed_ref.shape[1] - 16
    parts = mixed_ref.shape[0] // 2
    pair_residual(at_ref, (r0, r1, r2, r3), state_ref)
    cuts = (0, slice(0, 16)), (1, slice(tok - 16, tok))
    mixed = [
        jnp.concatenate([mixed_ref[k * parts + p, cut, :] for p in range(parts)], axis=1)
        for k, cut in cuts
    ]
    resid = [state_ref[0:16, :], state_ref[2 * tok - 16 : 2 * tok, :]]
    _, normed = normed_rows(
        jnp.concatenate(mixed),
        jnp.concatenate(resid),
        pair_gains(mixed_ref, tok),
        weight_ref[...],
        gain_ref[...],
    )
    normed = normed.astype(jnp.float32)
    first, last = normed[:1], normed[31:]
    even = jnp.full(first.shape, at_ref[3], jnp.int32) == 0
    near_ref[...] = jnp.where(even, last, first).astype(jnp.bfloat16)
    far_ref[...] = jnp.where(even, first, last).astype(jnp.bfloat16)


def rows_kernel(at_ref, mixed_ref, weight_ref, gain_ref, r0, r1, r2, r3, *refs):
    normed_ref, own_ref, state_ref = refs
    tok = mixed_ref.shape[1] - 16
    parts = mixed_ref.shape[0] // 2
    own = own_ref.shape[0]
    pair_residual(at_ref, (r0, r1, r2, r3), state_ref)
    gains = pair_gains(mixed_ref, tok)
    for k in range(2):
        cut = slice(k * tok, (k + 1) * tok)
        mixed = jnp.concatenate([mixed_ref[k * parts + p, :tok, :] for p in range(parts)], axis=1)
        state_ref[cut, :], normed_ref[cut, :] = normed_rows(
            mixed, state_ref[cut, :], gains, weight_ref[...], gain_ref[...]
        )
    start = (at_ref[0] * 8 + at_ref[1] * 2 + at_ref[2]) * own
    own_ref[...] = state_ref[pl.ds(pl.multiple_of(start, own), own), :]


def ffn_kernel(at_ref, cells_ref, near_ref, far_ref, vtap_ref, gtap_ref, *refs):
    line = refs[:8]
    keep_ref, send_ref, whole_ref, rows_ref, sums_ref = refs[8:]
    z = at_ref[0]
    tok, model = cells_ref.shape
    width = vtap_ref.shape[1]
    cut = line[0].shape[0]
    for d in range(8):
        start = pl.multiple_of(lax.rem(z + d, 8) * cut, cut)
        whole_ref[pl.ds(start, cut), :] = line[d][...]
    row = lax.broadcasted_iota(jnp.int32, (16, model), 0)
    even = jnp.full(row.shape, at_ref[1], jnp.int32) == 0
    near = jnp.broadcast_to(near_ref[...].astype(jnp.float32), row.shape)
    far = jnp.broadcast_to(far_ref[...].astype(jnp.float32), row.shape)
    after = jnp.where(even, near, far)
    before = jnp.where(even, far, near)
    tile = jnp.where(row == 0, after, jnp.where(row == 1, before, 0.0))
    rows_ref[:tok, :] = cells_ref[...]
    rows_ref[tok:, :] = tile.astype(jnp.bfloat16)
    both = jnp.dot(
        rows_ref[...], whole_ref[:, : 2 * width], preferred_element_type=jnp.float32
    )
    both = both.astype(jnp.bfloat16).astype(jnp.float32)

    def convolved(up, taps):
        mid, after, before = up[:tok], up[tok : tok + 1], up[tok + 1 : tok + 2]
        at = lax.broadcasted_iota(jnp.int32, mid.shape, 0)
        prev = jnp.where(at == 0, jnp.broadcast_to(before, mid.shape), pltpu.roll(mid, 1, 0))
        foll = jnp.where(
            at == tok - 1, jnp.broadcast_to(after, mid.shape), pltpu.roll(mid, tok - 1, 0)
        )
        return taps[0:1] * prev + taps[1:2] * mid + taps[2:3] * foll

    value = convolved(both[:, :width], vtap_ref[...])
    gate = convolved(both[:, width:], gtap_ref[...])
    hidden = (value * (gate / (1.0 + jnp.exp(-gate)))).astype(jnp.bfloat16)
    sums_ref[...] = lax.dot_general(
        hidden,
        whole_ref[:, 2 * width :],
        (((1,), (1,)), ((), ())),
        preferred_element_type=jnp.float32,
    ).astype(jnp.bfloat16)
    own = keep_ref.shape[1]
    core = at_ref[2]
    for p in range(keep_ref.shape[0]):
        start = pl.multiple_of((2 * p + core) * own, own)
        keep_ref[p] = sums_ref[pl.ds(start, own), :]
        start = pl.multiple_of((2 * p + 1 - core) * own, own)
        send_ref[p] = sums_ref[pl.ds(start, own), :]


def body(
    mixer_input,
    time_step,
    damping,
    input_map,
    readout,
    skip_gain,
    out_gain,
    out_weight,
    residual,
    channel_gain,
    value_weight,
    gate_weight,
    value_taps,
    gate_taps,
    down_weight,
):
    half = value_weight.shape[1] // 2
    packed = pl.pallas_call(
        pack_kernel,
        out_shape=jax.ShapeDtypeStruct((4, value_weight.shape[0], 3 * half), jnp.bfloat16),
        in_specs=[VMEM] * 3,
        out_specs=VMEM,
        name="pack",
    )(value_weight, gate_weight, down_weight.T)
    crossed = lax.all_to_all(packed, ("yh", "yl"), 0, 0, tiled=True)
    pieces = z_ring(crossed.reshape(-1, 3 * half))
    pair_resid = pair_rows(residual)
    mixed_y = mixer_branch(
        mixer_input, time_step, damping, input_map, readout, skip_gain, out_gain
    )
    tok_rows = mixer_input.shape[0]
    own_rows, model = residual.shape
    tp_count = lax.axis_size(TP)
    arrived = lax.all_to_all(mixed_y, PAIR, 0, 0, tiled=True)
    row_args = (
        jnp.stack([lax.axis_index(a) for a in (*PAIR, "yh")]).astype(jnp.int32),
        arrived,
        out_weight,
        channel_gain[None, :],
        *pair_resid,
    )
    state_scratch = [pltpu.VMEM((2 * tok_rows, model), jnp.bfloat16)]
    edge = jax.ShapeDtypeStruct((1, model), jnp.bfloat16)
    near, far = pl.pallas_call(
        edge_kernel,
        out_shape=(edge, edge),
        in_specs=[SMEM] + [VMEM] * 7,
        out_specs=(VMEM, VMEM),
        scratch_shapes=state_scratch,
        name="edge",
        cost_estimate=pl.CostEstimate(
            flops=300_000_000, bytes_accessed=6_000_000, transcendentals=0
        ),
    )(*row_args)
    near, far = edges_passed(near, far)
    cells, hidden_state = pl.pallas_call(
        rows_kernel,
        out_shape=(
            jax.ShapeDtypeStruct((2 * tok_rows, model), jnp.bfloat16),
            jax.ShapeDtypeStruct((own_rows, model), jnp.bfloat16),
        ),
        in_specs=[SMEM] + [VMEM] * 7,
        out_specs=(VMEM, VMEM),
        scratch_shapes=state_scratch,
        name="rows",
        cost_estimate=pl.CostEstimate(
            flops=1_000_000_000, bytes_accessed=6_000_000, transcendentals=0
        ),
    )(*row_args)
    state_wide = hidden_state.astype(jnp.float32)
    place = jnp.stack([lax.axis_index(a) for a in ("z", "yh", "c")]).astype(jnp.int32)
    shift = lax.axis_index("yl") * half
    taps = [lax.dynamic_slice(t, (0, shift), (3, half)) for t in (value_taps, gate_taps)]
    share = jax.ShapeDtypeStruct((tp_count, own_rows, model), jnp.bfloat16)
    keep, send = pl.pallas_call(
        ffn_kernel,
        out_shape=(share, share),
        in_specs=[SMEM] + [VMEM] * (5 + len(pieces)),
        out_specs=(VMEM, VMEM),
        scratch_shapes=[
            pltpu.VMEM((model, 3 * half), jnp.bfloat16),
            pltpu.VMEM((2 * tok_rows + 16, model), jnp.bfloat16),
            pltpu.VMEM((2 * tok_rows, model), jnp.bfloat16),
        ],
        name="ffn",
        cost_estimate=pl.CostEstimate(
            flops=1_300_000_000, bytes_accessed=6_000_000, transcendentals=100_000
        ),
    )(place, cells, near, far, *taps, *pieces)
    other = lax.ppermute(send, "c", [(0, 1), (1, 0)])
    both = (keep.astype(jnp.float32) + other.astype(jnp.float32)).astype(jnp.bfloat16)
    parts = lax.all_to_all(both, ("yl", "x"), 0, 0, tiled=True)
    summed = parts.astype(jnp.float32).sum(axis=0)
    return (state_wide + summed).astype(jnp.bfloat16)


def solution(mesh):
    fine = Mesh(mesh.devices.reshape(8, 2, 2, 4, 2), ("z", "yh", "yl", "x", "c"))
    in_specs = (
        P(SP, TP),
        P(None, TP),
        P(None, SP, TP),
        P(None, None, TP, None, None),
        P(None, None, TP, None, None),
        P(TP),
        P(TP),
        P(),
        P((*SP, *TP), None),
        P(),
        P(SP, TP),
        P(SP, TP),
        P(None, TP),
        P(None, TP),
        P(TP, SP),
    )
    out_specs = P((*SP, *TP), None)

    return jax.shard_map(body, mesh=fine, in_specs=in_specs, out_specs=out_specs, check_vma=False)
```

```python
import math

import jax
import jax.numpy as jnp
from jax import lax
from jax.experimental import pallas as pl
from jax.experimental.pallas import tpu as pltpu
from jax.sharding import Mesh
from jax.sharding import PartitionSpec as P


norm_eps = 1e-06
SP = ("z", "yh", "yl")
TP = ("x", "c")
PAIR = ("yl", "x", "c")
CHIPS = ("yl", "x")
VMEM = pl.BlockSpec(memory_space=pltpu.VMEM)
SMEM = pl.BlockSpec(memory_space=pltpu.SMEM)


def shifted(array, axis, step):
    n = lax.axis_size(axis)
    return lax.ppermute(array, axis, [(i, (i + step) % n) for i in range(n)])


def step_decays(table, damp_ref):
    rows = damp_ref.shape[2]
    half = damp_ref.shape[1], rows
    fwd = jnp.exp(-jnp.broadcast_to(table[3][:, :1], half) - damp_ref[0])
    bwd = jnp.exp(-jnp.broadcast_to(table[3][:, 64:65], half) - damp_ref[1])
    return fwd, bwd


def local_kernel(x_ref, table_ref, damp_ref, map_ref, end_ref, dre_ref, dim_ref):
    rows = x_ref.shape[0]
    groups = map_ref.shape[2]
    width = map_ref.shape[3]
    x = x_ref[...]
    scale = table_ref[2]
    owner = lax.broadcasted_iota(jnp.int32, (groups * width, 256), 0) // width
    for g in range(groups):
        block = jnp.concatenate(
            [map_ref[0, 0, g], map_ref[1, 0, g], map_ref[0, 1, g], map_ref[1, 1, g]], axis=1
        ).astype(jnp.float32)
        block = jnp.concatenate([block] * groups, axis=0)
        block = jnp.where(owner == g, block, 0.0).astype(jnp.bfloat16)
        drive = jnp.dot(x, block, preferred_element_type=jnp.float32)
        dre_ref[:, g, :] = drive[:, :128] * scale[g : g + 1, :]
        dim_ref[:, g, :] = drive[:, 128:] * scale[g : g + 1, :]
    cos, sin = table_ref[0], table_ref[1]
    lane_fwd = lax.broadcasted_iota(jnp.int32, (groups, 128), 1) < 64
    fwd, bwd = step_decays(table_ref, damp_ref)
    real = jnp.zeros((groups, 128), jnp.float32)
    imag = jnp.zeros((groups, 128), jnp.float32)
    for i in range(rows):
        j = rows - 1 - i
        size = jnp.where(
            lane_fwd,
            jnp.broadcast_to(fwd[:, i : i + 1], (groups, 128)),
            jnp.broadcast_to(bwd[:, j : j + 1], (groups, 128)),
        )
        dec_re, dec_im = size * cos, size * sin
        drive_re = jnp.where(lane_fwd, dre_ref[i], dre_ref[j])
        drive_im = jnp.where(lane_fwd, dim_ref[i], dim_ref[j])
        real, imag = (
            dec_re * real - dec_im * imag + drive_re,
            dec_re * imag + dec_im * real + drive_im,
        )
    total = jnp.sum(damp_ref[...], axis=2, keepdims=True)
    total = jnp.where(
        lane_fwd,
        jnp.broadcast_to(total[0], (groups, 128)),
        jnp.broadcast_to(total[1], (groups, 128)),
    )
    total = total + rows * table_ref[3]
    high = total.astype(jnp.bfloat16)
    low = (total - high.astype(jnp.float32)).astype(jnp.bfloat16).astype(jnp.float32)
    lane = lax.broadcasted_iota(jnp.int32, (groups, 128), 1)
    total = jnp.where(lane % 64 < 32, high.astype(jnp.float32), low).astype(jnp.bfloat16)
    real, imag = real.astype(jnp.bfloat16), imag.astype(jnp.bfloat16)
    for p in range(end_ref.shape[0]):
        end_ref[p, :, :128] = real
        end_ref[p, :, 128:256] = imag
        end_ref[p, :, 256:] = total


def mix_kernel(
    at_ref,
    ends_ref,
    dre_ref,
    dim_ref,
    table_ref,
    damp_ref,
    read_ref,
    x_ref,
    skip_ref,
    gain_ref,
    out_ref,
    fre_ref,
    fim_ref,
    bre_ref,
    bim_ref,
):
    rows = x_ref.shape[0]
    groups = dre_ref.shape[1]
    blocks = ends_ref.shape[0]
    at = at_ref[0]
    cos, sin = table_ref[0], table_ref[1]
    lane_fwd = lax.broadcasted_iota(jnp.int32, (groups, 128), 1) < 64
    block_re, block_im = cos, sin
    power = 1
    while power < rows:
        block_re, block_im = block_re * block_re - block_im * block_im, 2.0 * block_re * block_im
        power *= 2
    lane_high = lax.broadcasted_iota(jnp.int32, (groups, 128), 1) % 64 < 32

    def picked(i, j, at):
        fwd_part = ends_ref[i, :, at : at + 128].astype(jnp.float32)
        return jnp.where(lane_fwd, fwd_part, ends_ref[j, :, at : at + 128].astype(jnp.float32))

    real = jnp.zeros((groups, 128), jnp.float32)
    imag = jnp.zeros((groups, 128), jnp.float32)
    for i in range(blocks):
        j = blocks - 1 - i
        part = picked(i, j, 256)
        part = part + jnp.where(lane_high, pltpu.roll(part, 96, 1), pltpu.roll(part, 32, 1))
        size = jnp.exp(-part)
        dec_re, dec_im = size * block_re, size * block_im
        end_re, end_im = picked(i, j, 0), picked(i, j, 128)
        next_re = dec_re * real - dec_im * imag + end_re
        next_im = dec_re * imag + dec_im * real + end_im
        keep_fwd = jnp.where(i < at, 1, 0)
        keep_bwd = jnp.where(j > at, 1, 0)
        keep = jnp.where(lane_fwd, keep_fwd, keep_bwd) == 1
        real = jnp.where(keep, next_re, real)
        imag = jnp.where(keep, next_im, imag)
    fwd, bwd = step_decays(table_ref, damp_ref)
    for i in range(rows):
        j = rows - 1 - i
        size = jnp.where(
            lane_fwd,
            jnp.broadcast_to(fwd[:, i : i + 1], (groups, 128)),
            jnp.broadcast_to(bwd[:, j : j + 1], (groups, 128)),
        )
        dec_re, dec_im = size * cos, size * sin
        drive_re = jnp.where(lane_fwd, dre_ref[i], dre_ref[j])
        drive_im = jnp.where(lane_fwd, dim_ref[i], dim_ref[j])
        real, imag = (
            dec_re * real - dec_im * imag + drive_re,
            dec_re * imag + dec_im * real + drive_im,
        )
        fre_ref[i] = real
        fim_ref[i] = imag
        bre_ref[j] = real
        bim_ref[j] = imag
    width = read_ref.shape[3]
    channels = groups * width
    table = jnp.concatenate(
        [
            read_ref[0, 0].reshape(channels, 64),
            read_ref[1, 0].reshape(channels, 64),
            -read_ref[0, 1].reshape(channels, 64),
            -read_ref[1, 1].reshape(channels, 64),
        ],
        axis=1,
    )
    owner = lax.broadcasted_iota(jnp.int32, (channels, 256), 0) // width
    row_fwd = lax.broadcasted_iota(jnp.int32, (rows, 128), 1) < 64
    mixed = skip_ref[...] * x_ref[...].astype(jnp.float32)
    for g in range(groups):
        state = jnp.concatenate(
            [
                jnp.where(row_fwd, fre_ref[:, g, :], bre_ref[:, g, :]),
                jnp.where(row_fwd, fim_ref[:, g, :], bim_ref[:, g, :]),
            ],
            axis=1,
        ).astype(jnp.bfloat16)
        part = jnp.where(owner == g, table, 0.0).astype(jnp.bfloat16)
        mixed = mixed + lax.dot_general(
            state, part, (((1,), (1,)), ((), ())), preferred_element_type=jnp.float32
        )
    high = gain_ref[...].astype(jnp.bfloat16).astype(jnp.float32)
    mid = (gain_ref[...] - high).astype(jnp.bfloat16).astype(jnp.float32)
    low = gain_ref[...] - high - mid
    row = lax.broadcasted_iota(jnp.int32, (16, channels), 0)
    tail = jnp.zeros(row.shape, jnp.float32)
    for k, part in enumerate((high, mid, low)):
        tail = jnp.where(row == k, jnp.broadcast_to(part, row.shape), tail)
    mixed, tail = mixed.astype(jnp.bfloat16), tail.astype(jnp.bfloat16)
    for p in range(out_ref.shape[0]):
        out_ref[p, :rows, :] = mixed
        out_ref[p, rows:, :] = tail


def mixer_branch(mixer_input, time_step, damping, input_map, readout, skip_gain, out_gain):
    rows = mixer_input.shape[0]
    groups = time_step.shape[1]
    states = input_map.shape[3]
    frequency = math.pi * jnp.arange(states, dtype=jnp.float32)
    step = time_step.T[:, :, None]
    shape = (groups, 2, states)
    rotation = step * frequency
    table = jnp.stack(
        [
            jnp.cos(rotation),
            jnp.sin(rotation),
            jnp.broadcast_to(jnp.sqrt(-jnp.expm1(-step)), shape),
            jnp.broadcast_to(0.5 * step, shape),
        ]
    ).reshape(4, groups, 2 * states)
    damp = jnp.swapaxes(damping, 1, 2)
    maps = jnp.swapaxes(input_map, 3, 4)
    drive_shape = jax.ShapeDtypeStruct((rows, groups, 2 * states), jnp.float32)
    ends, drive_re, drive_im = pl.pallas_call(
        local_kernel,
        out_shape=(
            jax.ShapeDtypeStruct((lax.axis_size(SP), groups, 6 * states), jnp.bfloat16),
            drive_shape,
            drive_shape,
        ),
        in_specs=[VMEM] * 4,
        out_specs=(VMEM,) * 3,
        name="mixer_local",
        cost_estimate=pl.CostEstimate(
            flops=300_000_000, bytes_accessed=2_000_000, transcendentals=0
        ),
    )(mixer_input, table, damp, maps)
    all_ends = lax.all_to_all(ends, SP, 0, 0, tiled=True)
    at = lax.axis_index(SP).astype(jnp.int32).reshape(1)
    scratch = pltpu.VMEM((rows, groups, 2 * states), jnp.float32)
    copies = lax.axis_size(CHIPS)
    return pl.pallas_call(
        mix_kernel,
        out_shape=jax.ShapeDtypeStruct(
            (copies, rows + 16, mixer_input.shape[1]), jnp.bfloat16
        ),
        in_specs=[SMEM] + [VMEM] * 9,
        out_specs=VMEM,
        scratch_shapes=[scratch] * 4,
        name="mixer_out",
        cost_estimate=pl.CostEstimate(
            flops=300_000_000, bytes_accessed=2_000_000, transcendentals=0
        ),
    )(
        at,
        all_ends,
        drive_re,
        drive_im,
        table,
        damp,
        readout,
        mixer_input,
        skip_gain[None, :],
        out_gain[None, :],
    )


def z_ring(block):
    found = {0: block}
    up = down = block
    for s in range(1, 5):
        found[8 - s] = up = shifted(up, "z", 1)
        if s < 4:
            found[s] = down = shifted(down, "z", -1)
    return [found[d] for d in range(8)]


def pair_rows(rows):
    both = jnp.stack((rows, lax.ppermute(rows, "yl", [(0, 1), (1, 0)])))
    quad = jnp.concatenate((both, lax.ppermute(both, "c", [(0, 1), (1, 0)])))
    pieces = {0: quad}
    for d in (1, 3, 2):
        pieces[d] = shifted(quad, "x", -d)
    return [pieces[d] for d in range(4)]


def edges_passed(near, far):
    pairs = [(2 * i + 1, 2 * i + 2) for i in range(lax.axis_size("z") - 1)]
    far = lax.ppermute(far, ("z", "yh"), pairs + [(j, i) for i, j in pairs])
    near = lax.ppermute(near, "yh", [(0, 1), (1, 0)])
    return near, far


def pack_kernel(value_ref, gate_ref, down_ref, out_ref):
    half = value_ref.shape[1] // 2
    for k in range(out_ref.shape[0]):
        cut = slice(k % 2 * half, (k % 2 + 1) * half)
        out_ref[k, :, :half] = value_ref[:, cut]
        out_ref[k, :, half : 2 * half] = gate_ref[:, cut]
        out_ref[k, :, 2 * half :] = down_ref[:, cut]


def pair_mixed(at_ref, own_ref, beside_ref, k, cut):
    parts = []
    for x in range(4):
        own = own_ref[4 * k + x, cut, :].astype(jnp.float32)
        beside = beside_ref[4 * k + x, cut, :].astype(jnp.float32)
        north = jnp.full(own.shape, at_ref[2], jnp.int32) == 1
        parts += [jnp.where(north, beside, own), jnp.where(north, own, beside)]
    return jnp.concatenate(parts, axis=1)


def pair_gains(at_ref, own_ref, beside_ref, tok):
    g = pair_mixed(at_ref, own_ref, beside_ref, 0, slice(tok, tok + 16))
    return g[0:1] + g[1:2] + g[2:3]


def pair_residual(at_ref, pieces, state_ref):
    low, x, core = at_ref[0], at_ref[1], at_ref[2]
    own = pieces[0].shape[1]
    for dx, ref in enumerate(pieces):
        for k in range(4):
            row = lax.rem(low + k % 2, 2) * 8 + lax.rem(x + dx, 4) * 2 + lax.rem(core + k // 2, 2)
            state_ref[pl.ds(pl.multiple_of(row * own, own), own), :] = ref[k]


def normed_rows(mixed, resid, gains, weight, gain):
    inverse = lax.rsqrt(jnp.mean(mixed * mixed, axis=1, keepdims=True) + norm_eps)
    normed_mix = (mixed * inverse * gains).astype(jnp.bfloat16)
    added = jnp.dot(normed_mix, weight, preferred_element_type=jnp.float32)
    state = (resid.astype(jnp.float32) + added).astype(jnp.bfloat16)
    wide = state.astype(jnp.float32)
    scale = lax.rsqrt(jnp.mean(wide * wide, axis=1, keepdims=True) + norm_eps)
    return state, (wide * scale * gain).astype(jnp.bfloat16)


def edge_kernel(at_ref, mixed_ref, beside_ref, weight_ref, gain_ref, r0, r1, r2, r3, *refs):
    near_ref, far_ref, state_ref = refs
    tok = mixed_ref.shape[1] - 16
    pair_residual(at_ref, (r0, r1, r2, r3), state_ref)
    cuts = (0, slice(0, 16)), (1, slice(tok - 16, tok))
    mixed = [pair_mixed(at_ref, mixed_ref, beside_ref, k, cut) for k, cut in cuts]
    resid = [state_ref[0:16, :], state_ref[2 * tok - 16 : 2 * tok, :]]
    _, normed = normed_rows(
        jnp.concatenate(mixed),
        jnp.concatenate(resid),
        pair_gains(at_ref, mixed_ref, beside_ref, tok),
        weight_ref[...],
        gain_ref[...],
    )
    normed = normed.astype(jnp.float32)
    first, last = normed[:1], normed[31:]
    even = jnp.full(first.shape, at_ref[3], jnp.int32) == 0
    near_ref[...] = jnp.where(even, last, first).astype(jnp.bfloat16)
    far_ref[...] = jnp.where(even, first, last).astype(jnp.bfloat16)


def rows_kernel(at_ref, mixed_ref, beside_ref, weight_ref, gain_ref, r0, r1, r2, r3, *refs):
    normed_ref, own_ref, state_ref = refs
    tok = mixed_ref.shape[1] - 16
    own = own_ref.shape[0]
    pair_residual(at_ref, (r0, r1, r2, r3), state_ref)
    gains = pair_gains(at_ref, mixed_ref, beside_ref, tok)
    for k in range(2):
        cut = slice(k * tok, (k + 1) * tok)
        mixed = pair_mixed(at_ref, mixed_ref, beside_ref, k, slice(0, tok))
        state_ref[cut, :], normed_ref[cut, :] = normed_rows(
            mixed, state_ref[cut, :], gains, weight_ref[...], gain_ref[...]
        )
    start = (at_ref[0] * 8 + at_ref[1] * 2 + at_ref[2]) * own
    own_ref[...] = state_ref[pl.ds(pl.multiple_of(start, own), own), :]


def ffn_kernel(at_ref, cells_ref, near_ref, far_ref, vtap_ref, gtap_ref, *refs):
    line = refs[:8]
    keep_ref, send_ref, whole_ref, rows_ref, sums_ref = refs[8:]
    z = at_ref[0]
    tok, model = cells_ref.shape
    width = vtap_ref.shape[1]
    cut = line[0].shape[0]
    for d in range(8):
        start = pl.multiple_of(lax.rem(z + d, 8) * cut, cut)
        whole_ref[pl.ds(start, cut), :] = line[d][...]
    row = lax.broadcasted_iota(jnp.int32, (16, model), 0)
    even = jnp.full(row.shape, at_ref[1], jnp.int32) == 0
    near = jnp.broadcast_to(near_ref[...].astype(jnp.float32), row.shape)
    far = jnp.broadcast_to(far_ref[...].astype(jnp.float32), row.shape)
    after = jnp.where(even, near, far)
    before = jnp.where(even, far, near)
    tile = jnp.where(row == 0, after, jnp.where(row == 1, before, 0.0))
    rows_ref[:tok, :] = cells_ref[...]
    rows_ref[tok:, :] = tile.astype(jnp.bfloat16)
    both = jnp.dot(
        rows_ref[...], whole_ref[:, : 2 * width], preferred_element_type=jnp.float32
    )
    both = both.astype(jnp.bfloat16).astype(jnp.float32)

    def convolved(up, taps):
        mid, after, before = up[:tok], up[tok : tok + 1], up[tok + 1 : tok + 2]
        at = lax.broadcasted_iota(jnp.int32, mid.shape, 0)
        prev = jnp.where(at == 0, jnp.broadcast_to(before, mid.shape), pltpu.roll(mid, 1, 0))
        foll = jnp.where(
            at == tok - 1, jnp.broadcast_to(after, mid.shape), pltpu.roll(mid, tok - 1, 0)
        )
        return taps[0:1] * prev + taps[1:2] * mid + taps[2:3] * foll

    value = convolved(both[:, :width], vtap_ref[...])
    gate = convolved(both[:, width:], gtap_ref[...])
    hidden = (value * (gate / (1.0 + jnp.exp(-gate)))).astype(jnp.bfloat16)
    sums_ref[...] = lax.dot_general(
        hidden,
        whole_ref[:, 2 * width :],
        (((1,), (1,)), ((), ())),
        preferred_element_type=jnp.float32,
    ).astype(jnp.bfloat16)
    own = keep_ref.shape[1]
    core = at_ref[2]
    for p in range(keep_ref.shape[0]):
        start = pl.multiple_of((2 * p + core) * own, own)
        keep_ref[p] = sums_ref[pl.ds(start, own), :]
        start = pl.multiple_of((2 * p + 1 - core) * own, own)
        send_ref[p] = sums_ref[pl.ds(start, own), :]


def body(
    mixer_input,
    time_step,
    damping,
    input_map,
    readout,
    skip_gain,
    out_gain,
    out_weight,
    residual,
    channel_gain,
    value_weight,
    gate_weight,
    value_taps,
    gate_taps,
    down_weight,
):
    half = value_weight.shape[1] // 2
    packed = pl.pallas_call(
        pack_kernel,
        out_shape=jax.ShapeDtypeStruct((4, value_weight.shape[0], 3 * half), jnp.bfloat16),
        in_specs=[VMEM] * 3,
        out_specs=VMEM,
        name="pack",
    )(value_weight, gate_weight, down_weight.T)
    crossed = lax.all_to_all(packed, ("yh", "yl"), 0, 0, tiled=True)
    pieces = z_ring(crossed.reshape(-1, 3 * half))
    pair_resid = pair_rows(residual)
    mixed_y = mixer_branch(
        mixer_input, time_step, damping, input_map, readout, skip_gain, out_gain
    )
    tok_rows = mixer_input.shape[0]
    own_rows, model = residual.shape
    tp_count = lax.axis_size(TP)
    arrived = lax.all_to_all(mixed_y, CHIPS, 0, 0, tiled=True)
    beside = lax.ppermute(arrived, "c", [(0, 1), (1, 0)])
    row_args = (
        jnp.stack([lax.axis_index(a) for a in (*PAIR, "yh")]).astype(jnp.int32),
        arrived,
        beside,
        out_weight,
        channel_gain[None, :],
        *pair_resid,
    )
    state_scratch = [pltpu.VMEM((2 * tok_rows, model), jnp.bfloat16)]
    edge = jax.ShapeDtypeStruct((1, model), jnp.bfloat16)
    near, far = pl.pallas_call(
        edge_kernel,
        out_shape=(edge, edge),
        in_specs=[SMEM] + [VMEM] * 8,
        out_specs=(VMEM, VMEM),
        scratch_shapes=state_scratch,
        name="edge",
compiler_params=pltpu.CompilerParams(vmem_limit_bytes=16 * 2**20),
        cost_estimate=pl.CostEstimate(
            flops=300_000_000, bytes_accessed=6_000_000, transcendentals=0
        ),
    )(*row_args)
    near, far = edges_passed(near, far)
    cells, hidden_state = pl.pallas_call(
        rows_kernel,
        out_shape=(
            jax.ShapeDtypeStruct((2 * tok_rows, model), jnp.bfloat16),
            jax.ShapeDtypeStruct((own_rows, model), jnp.bfloat16),
        ),
        in_specs=[SMEM] + [VMEM] * 8,
        out_specs=(VMEM, VMEM),
        scratch_shapes=state_scratch,
        name="rows",
compiler_params=pltpu.CompilerParams(vmem_limit_bytes=20 * 2**20),
        cost_estimate=pl.CostEstimate(
            flops=1_000_000_000, bytes_accessed=6_000_000, transcendentals=0
        ),
    )(*row_args)
    state_wide = hidden_state.astype(jnp.float32)
    place = jnp.stack([lax.axis_index(a) for a in ("z", "yh", "c")]).astype(jnp.int32)
    shift = lax.axis_index("yl") * half
    taps = [lax.dynamic_slice(t, (0, shift), (3, half)) for t in (value_taps, gate_taps)]
    share = jax.ShapeDtypeStruct((tp_count, own_rows, model), jnp.bfloat16)
    keep, send = pl.pallas_call(
        ffn_kernel,
        out_shape=(share, share),
        in_specs=[SMEM] + [VMEM] * (5 + len(pieces)),
        out_specs=(VMEM, VMEM),
        scratch_shapes=[
            pltpu.VMEM((model, 3 * half), jnp.bfloat16),
            pltpu.VMEM((2 * tok_rows + 16, model), jnp.bfloat16),
            pltpu.VMEM((2 * tok_rows, model), jnp.bfloat16),
        ],
        name="ffn",
compiler_params=pltpu.CompilerParams(vmem_limit_bytes=26 * 2**20),
        cost_estimate=pl.CostEstimate(
            flops=1_300_000_000, bytes_accessed=6_000_000, transcendentals=100_000
        ),
    )(place, cells, near, far, *taps, *pieces)
    other = lax.ppermute(send, "c", [(0, 1), (1, 0)])
    both = (keep.astype(jnp.float32) + other.astype(jnp.float32)).astype(jnp.bfloat16)
    parts = lax.all_to_all(both, CHIPS, 0, 0, tiled=True)
    summed = parts.astype(jnp.float32).sum(axis=0)
    return (state_wide + summed).astype(jnp.bfloat16)


def solution(mesh):
    fine = Mesh(mesh.devices.reshape(8, 2, 2, 4, 2), ("z", "yh", "yl", "x", "c"))
    in_specs = (
        P(SP, TP),
        P(None, TP),
        P(None, SP, TP),
        P(None, None, TP, None, None),
        P(None, None, TP, None, None),
        P(TP),
        P(TP),
        P(),
        P((*SP, *TP), None),
        P(),
        P(SP, TP),
        P(SP, TP),
        P(None, TP),
        P(None, TP),
        P(TP, SP),
    )
    out_specs = P((*SP, *TP), None)

    return jax.shard_map(body, mesh=fine, in_specs=in_specs, out_specs=out_specs, check_vma=False)
```

```python
import math

import jax
import jax.numpy as jnp
from jax import lax
from jax.experimental import pallas as pl
from jax.experimental.pallas import tpu as pltpu
from jax.sharding import Mesh
from jax.sharding import PartitionSpec as P


norm_eps = 1e-06
SP = ("z", "yh", "yl")
TP = ("x", "c")
PAIR = ("yl", "x", "c")
CHIPS = ("yl", "x")
VMEM = pl.BlockSpec(memory_space=pltpu.VMEM)
SMEM = pl.BlockSpec(memory_space=pltpu.SMEM)


def shifted(array, axis, step):
    n = lax.axis_size(axis)
    return lax.ppermute(array, axis, [(i, (i + step) % n) for i in range(n)])


def step_decays(table, damp_ref):
    rows = damp_ref.shape[2]
    half = damp_ref.shape[1], rows
    fwd = jnp.exp(-jnp.broadcast_to(table[3][:, :1], half) - damp_ref[0])
    bwd = jnp.exp(-jnp.broadcast_to(table[3][:, 64:65], half) - damp_ref[1])
    return fwd, bwd


def local_kernel(x_ref, table_ref, damp_ref, map_ref, end_ref, dre_ref, dim_ref):
    rows = x_ref.shape[0]
    groups = map_ref.shape[2]
    width = map_ref.shape[3]
    x = x_ref[...]
    scale = table_ref[2]
    owner = lax.broadcasted_iota(jnp.int32, (groups * width, 256), 0) // width
    for g in range(groups):
        block = jnp.concatenate(
            [map_ref[0, 0, g], map_ref[1, 0, g], map_ref[0, 1, g], map_ref[1, 1, g]], axis=1
        ).astype(jnp.float32)
        block = jnp.concatenate([block] * groups, axis=0)
        block = jnp.where(owner == g, block, 0.0).astype(jnp.bfloat16)
        drive = jnp.dot(x, block, preferred_element_type=jnp.float32)
        dre_ref[:, g, :] = drive[:, :128] * scale[g : g + 1, :]
        dim_ref[:, g, :] = drive[:, 128:] * scale[g : g + 1, :]
    cos, sin = table_ref[0], table_ref[1]
    lane_fwd = lax.broadcasted_iota(jnp.int32, (groups, 128), 1) < 64
    fwd, bwd = step_decays(table_ref, damp_ref)
    real = jnp.zeros((groups, 128), jnp.float32)
    imag = jnp.zeros((groups, 128), jnp.float32)
    for i in range(rows):
        j = rows - 1 - i
        size = jnp.where(
            lane_fwd,
            jnp.broadcast_to(fwd[:, i : i + 1], (groups, 128)),
            jnp.broadcast_to(bwd[:, j : j + 1], (groups, 128)),
        )
        dec_re, dec_im = size * cos, size * sin
        drive_re = jnp.where(lane_fwd, dre_ref[i], dre_ref[j])
        drive_im = jnp.where(lane_fwd, dim_ref[i], dim_ref[j])
        real, imag = (
            dec_re * real - dec_im * imag + drive_re,
            dec_re * imag + dec_im * real + drive_im,
        )
    total = jnp.sum(damp_ref[...], axis=2, keepdims=True)
    total = jnp.where(
        lane_fwd,
        jnp.broadcast_to(total[0], (groups, 128)),
        jnp.broadcast_to(total[1], (groups, 128)),
    )
    total = total + rows * table_ref[3]
    high = total.astype(jnp.bfloat16)
    low = (total - high.astype(jnp.float32)).astype(jnp.bfloat16).astype(jnp.float32)
    lane = lax.broadcasted_iota(jnp.int32, (groups, 128), 1)
    total = jnp.where(lane % 64 < 32, high.astype(jnp.float32), low).astype(jnp.bfloat16)
    real, imag = real.astype(jnp.bfloat16), imag.astype(jnp.bfloat16)
    for p in range(end_ref.shape[0]):
        end_ref[p, :, :128] = real
        end_ref[p, :, 128:256] = imag
        end_ref[p, :, 256:] = total


def mix_kernel(
    at_ref,
    ends_ref,
    dre_ref,
    dim_ref,
    table_ref,
    damp_ref,
    read_ref,
    x_ref,
    skip_ref,
    gain_ref,
    out_ref,
    fre_ref,
    fim_ref,
    bre_ref,
    bim_ref,
):
    rows = x_ref.shape[0]
    groups = dre_ref.shape[1]
    blocks = ends_ref.shape[0]
    at = at_ref[0]
    cos, sin = table_ref[0], table_ref[1]
    lane_fwd = lax.broadcasted_iota(jnp.int32, (groups, 128), 1) < 64
    block_re, block_im = cos, sin
    power = 1
    while power < rows:
        block_re, block_im = block_re * block_re - block_im * block_im, 2.0 * block_re * block_im
        power *= 2
    lane_high = lax.broadcasted_iota(jnp.int32, (groups, 128), 1) % 64 < 32

    def picked(i, j, at):
        fwd_part = ends_ref[i, :, at : at + 128].astype(jnp.float32)
        return jnp.where(lane_fwd, fwd_part, ends_ref[j, :, at : at + 128].astype(jnp.float32))

    real = jnp.zeros((groups, 128), jnp.float32)
    imag = jnp.zeros((groups, 128), jnp.float32)
    for i in range(blocks):
        j = blocks - 1 - i
        part = picked(i, j, 256)
        part = part + jnp.where(lane_high, pltpu.roll(part, 96, 1), pltpu.roll(part, 32, 1))
        size = jnp.exp(-part)
        dec_re, dec_im = size * block_re, size * block_im
        end_re, end_im = picked(i, j, 0), picked(i, j, 128)
        next_re = dec_re * real - dec_im * imag + end_re
        next_im = dec_re * imag + dec_im * real + end_im
        keep_fwd = jnp.where(i < at, 1, 0)
        keep_bwd = jnp.where(j > at, 1, 0)
        keep = jnp.where(lane_fwd, keep_fwd, keep_bwd) == 1
        real = jnp.where(keep, next_re, real)
        imag = jnp.where(keep, next_im, imag)
    fwd, bwd = step_decays(table_ref, damp_ref)
    for i in range(rows):
        j = rows - 1 - i
        size = jnp.where(
            lane_fwd,
            jnp.broadcast_to(fwd[:, i : i + 1], (groups, 128)),
            jnp.broadcast_to(bwd[:, j : j + 1], (groups, 128)),
        )
        dec_re, dec_im = size * cos, size * sin
        drive_re = jnp.where(lane_fwd, dre_ref[i], dre_ref[j])
        drive_im = jnp.where(lane_fwd, dim_ref[i], dim_ref[j])
        real, imag = (
            dec_re * real - dec_im * imag + drive_re,
            dec_re * imag + dec_im * real + drive_im,
        )
        fre_ref[i] = real
        fim_ref[i] = imag
        bre_ref[j] = real
        bim_ref[j] = imag
    width = read_ref.shape[3]
    channels = groups * width
    table = jnp.concatenate(
        [
            read_ref[0, 0].reshape(channels, 64),
            read_ref[1, 0].reshape(channels, 64),
            -read_ref[0, 1].reshape(channels, 64),
            -read_ref[1, 1].reshape(channels, 64),
        ],
        axis=1,
    )
    owner = lax.broadcasted_iota(jnp.int32, (channels, 256), 0) // width
    row_fwd = lax.broadcasted_iota(jnp.int32, (rows, 128), 1) < 64
    mixed = skip_ref[...] * x_ref[...].astype(jnp.float32)
    for g in range(groups):
        state = jnp.concatenate(
            [
                jnp.where(row_fwd, fre_ref[:, g, :], bre_ref[:, g, :]),
                jnp.where(row_fwd, fim_ref[:, g, :], bim_ref[:, g, :]),
            ],
            axis=1,
        ).astype(jnp.bfloat16)
        part = jnp.where(owner == g, table, 0.0).astype(jnp.bfloat16)
        mixed = mixed + lax.dot_general(
            state, part, (((1,), (1,)), ((), ())), preferred_element_type=jnp.float32
        )
    high = gain_ref[...].astype(jnp.bfloat16).astype(jnp.float32)
    mid = (gain_ref[...] - high).astype(jnp.bfloat16).astype(jnp.float32)
    low = gain_ref[...] - high - mid
    row = lax.broadcasted_iota(jnp.int32, (8, channels), 0)
    tail = jnp.zeros(row.shape, jnp.float32)
    for k, part in enumerate((high, mid, low)):
        tail = jnp.where(row == k, jnp.broadcast_to(part, row.shape), tail)
    mixed, tail = mixed.astype(jnp.bfloat16), tail.astype(jnp.bfloat16)
    for p in range(out_ref.shape[0]):
        out_ref[p, :rows, :] = mixed
        out_ref[p, rows:, :] = tail


def mixer_branch(mixer_input, time_step, damping, input_map, readout, skip_gain, out_gain):
    rows = mixer_input.shape[0]
    groups = time_step.shape[1]
    states = input_map.shape[3]
    frequency = math.pi * jnp.arange(states, dtype=jnp.float32)
    step = time_step.T[:, :, None]
    shape = (groups, 2, states)
    rotation = step * frequency
    table = jnp.stack(
        [
            jnp.cos(rotation),
            jnp.sin(rotation),
            jnp.broadcast_to(jnp.sqrt(-jnp.expm1(-step)), shape),
            jnp.broadcast_to(0.5 * step, shape),
        ]
    ).reshape(4, groups, 2 * states)
    damp = jnp.swapaxes(damping, 1, 2)
    maps = jnp.swapaxes(input_map, 3, 4)
    drive_shape = jax.ShapeDtypeStruct((rows, groups, 2 * states), jnp.float32)
    ends, drive_re, drive_im = pl.pallas_call(
        local_kernel,
        out_shape=(
            jax.ShapeDtypeStruct((lax.axis_size(SP), groups, 6 * states), jnp.bfloat16),
            drive_shape,
            drive_shape,
        ),
        in_specs=[VMEM] * 4,
        out_specs=(VMEM,) * 3,
        name="mixer_local",
        cost_estimate=pl.CostEstimate(
            flops=300_000_000, bytes_accessed=2_000_000, transcendentals=0
        ),
    )(mixer_input, table, damp, maps)
    all_ends = lax.all_to_all(ends, SP, 0, 0, tiled=True)
    at = lax.axis_index(SP).astype(jnp.int32).reshape(1)
    scratch = pltpu.VMEM((rows, groups, 2 * states), jnp.float32)
    copies = lax.axis_size(CHIPS)
    return pl.pallas_call(
        mix_kernel,
        out_shape=jax.ShapeDtypeStruct(
            (copies, rows + 8, mixer_input.shape[1]), jnp.bfloat16
        ),
        in_specs=[SMEM] + [VMEM] * 9,
        out_specs=VMEM,
        scratch_shapes=[scratch] * 4,
        name="mixer_out",
        cost_estimate=pl.CostEstimate(
            flops=300_000_000, bytes_accessed=2_000_000, transcendentals=0
        ),
    )(
        at,
        all_ends,
        drive_re,
        drive_im,
        table,
        damp,
        readout,
        mixer_input,
        skip_gain[None, :],
        out_gain[None, :],
    )


def z_ring(block):
    found = {0: block}
    up = down = block
    for s in range(1, 5):
        found[8 - s] = up = shifted(up, "z", 1)
        if s < 4:
            found[s] = down = shifted(down, "z", -1)
    return [found[d] for d in range(8)]


def pair_rows(rows):
    both = jnp.stack((rows, lax.ppermute(rows, "yl", [(0, 1), (1, 0)])))
    quad = jnp.concatenate((both, lax.ppermute(both, "c", [(0, 1), (1, 0)])))
    pieces = {0: quad}
    for d in (1, 3, 2):
        pieces[d] = shifted(quad, "x", -d)
    return [pieces[d] for d in range(4)]


def edges_passed(near, far):
    pairs = [(2 * i + 1, 2 * i + 2) for i in range(lax.axis_size("z") - 1)]
    far = lax.ppermute(far, ("z", "yh"), pairs + [(j, i) for i, j in pairs])
    near = lax.ppermute(near, "yh", [(0, 1), (1, 0)])
    return near, far


def pack_kernel(value_ref, gate_ref, down_ref, out_ref):
    half = value_ref.shape[1] // 2
    for k in range(out_ref.shape[0]):
        cut = slice(k % 2 * half, (k % 2 + 1) * half)
        out_ref[k, :, :half] = value_ref[:, cut]
        out_ref[k, :, half : 2 * half] = gate_ref[:, cut]
        out_ref[k, :, 2 * half :] = down_ref[:, cut]


def pair_mixed(at_ref, own_ref, beside_ref, k, cut):
    parts = []
    for x in range(4):
        own = own_ref[4 * k + x, cut, :].astype(jnp.float32)
        beside = beside_ref[4 * k + x, cut, :].astype(jnp.float32)
        north = jnp.full(own.shape, at_ref[2], jnp.int32) == 1
        parts += [jnp.where(north, beside, own), jnp.where(north, own, beside)]
    return jnp.concatenate(parts, axis=1)


def pair_gains(at_ref, own_ref, beside_ref, tok):
    g = pair_mixed(at_ref, own_ref, beside_ref, 0, slice(tok, tok + 8))
    return g[0:1] + g[1:2] + g[2:3]


def pair_residual(at_ref, pieces, state_ref):
    low, x, core = at_ref[0], at_ref[1], at_ref[2]
    own = pieces[0].shape[1]
    for dx, ref in enumerate(pieces):
        for k in range(4):
            row = lax.rem(low + k % 2, 2) * 8 + lax.rem(x + dx, 4) * 2 + lax.rem(core + k // 2, 2)
            state_ref[pl.ds(pl.multiple_of(row * own, own), own), :] = ref[k]


def normed_rows(mixed, resid, gains, weight, gain):
    inverse = lax.rsqrt(jnp.mean(mixed * mixed, axis=1, keepdims=True) + norm_eps)
    normed_mix = (mixed * inverse * gains).astype(jnp.bfloat16)
    added = jnp.dot(normed_mix, weight, preferred_element_type=jnp.float32)
    state = (resid.astype(jnp.float32) + added).astype(jnp.bfloat16)
    wide = state.astype(jnp.float32)
    scale = lax.rsqrt(jnp.mean(wide * wide, axis=1, keepdims=True) + norm_eps)
    return state, (wide * scale * gain).astype(jnp.bfloat16)


def edge_kernel(at_ref, mixed_ref, beside_ref, weight_ref, gain_ref, r0, r1, r2, r3, *refs):
    near_ref, far_ref, state_ref = refs
    tok = mixed_ref.shape[1] - 8
    pair_residual(at_ref, (r0, r1, r2, r3), state_ref)
    cuts = (0, slice(0, 16)), (1, slice(tok - 16, tok))
    mixed = [pair_mixed(at_ref, mixed_ref, beside_ref, k, cut) for k, cut in cuts]
    resid = [state_ref[0:16, :], state_ref[2 * tok - 16 : 2 * tok, :]]
    _, normed = normed_rows(
        jnp.concatenate(mixed),
        jnp.concatenate(resid),
        pair_gains(at_ref, mixed_ref, beside_ref, tok),
        weight_ref[...],
        gain_ref[...],
    )
    normed = normed.astype(jnp.float32)
    first, last = normed[:1], normed[31:]
    even = jnp.full(first.shape, at_ref[3], jnp.int32) == 0
    near_ref[...] = jnp.where(even, last, first).astype(jnp.bfloat16)
    far_ref[...] = jnp.where(even, first, last).astype(jnp.bfloat16)


def rows_kernel(at_ref, mixed_ref, beside_ref, weight_ref, gain_ref, r0, r1, r2, r3, *refs):
    normed_ref, own_ref, state_ref = refs
    tok = mixed_ref.shape[1] - 8
    own = own_ref.shape[0]
    pair_residual(at_ref, (r0, r1, r2, r3), state_ref)
    gains = pair_gains(at_ref, mixed_ref, beside_ref, tok)
    for k in range(2):
        cut = slice(k * tok, (k + 1) * tok)
        mixed = pair_mixed(at_ref, mixed_ref, beside_ref, k, slice(0, tok))
        state_ref[cut, :], normed_ref[cut, :] = normed_rows(
            mixed, state_ref[cut, :], gains, weight_ref[...], gain_ref[...]
        )
    start = (at_ref[0] * 8 + at_ref[1] * 2 + at_ref[2]) * own
    own_ref[...] = state_ref[pl.ds(pl.multiple_of(start, own), own), :]


def ffn_kernel(at_ref, cells_ref, near_ref, far_ref, vtap_ref, gtap_ref, *refs):
    line = refs[:8]
    keep_ref, send_ref, whole_ref, rows_ref, sums_ref = refs[8:]
    z = at_ref[0]
    tok, model = cells_ref.shape
    width = vtap_ref.shape[1]
    cut = line[0].shape[0]
    for d in range(8):
        start = pl.multiple_of(lax.rem(z + d, 8) * cut, cut)
        whole_ref[pl.ds(start, cut), :] = line[d][...]
    row = lax.broadcasted_iota(jnp.int32, (16, model), 0)
    even = jnp.full(row.shape, at_ref[1], jnp.int32) == 0
    near = jnp.broadcast_to(near_ref[...].astype(jnp.float32), row.shape)
    far = jnp.broadcast_to(far_ref[...].astype(jnp.float32), row.shape)
    after = jnp.where(even, near, far)
    before = jnp.where(even, far, near)
    tile = jnp.where(row == 0, after, jnp.where(row == 1, before, 0.0))
    rows_ref[:tok, :] = cells_ref[...]
    rows_ref[tok:, :] = tile.astype(jnp.bfloat16)
    both = jnp.dot(
        rows_ref[...], whole_ref[:, : 2 * width], preferred_element_type=jnp.float32
    )
    both = both.astype(jnp.bfloat16).astype(jnp.float32)

    def convolved(up, taps):
        mid, after, before = up[:tok], up[tok : tok + 1], up[tok + 1 : tok + 2]
        at = lax.broadcasted_iota(jnp.int32, mid.shape, 0)
        prev = jnp.where(at == 0, jnp.broadcast_to(before, mid.shape), pltpu.roll(mid, 1, 0))
        foll = jnp.where(
            at == tok - 1, jnp.broadcast_to(after, mid.shape), pltpu.roll(mid, tok - 1, 0)
        )
        return taps[0:1] * prev + taps[1:2] * mid + taps[2:3] * foll

    value = convolved(both[:, :width], vtap_ref[...])
    gate = convolved(both[:, width:], gtap_ref[...])
    hidden = (value * (gate / (1.0 + jnp.exp(-gate)))).astype(jnp.bfloat16)
    sums_ref[...] = lax.dot_general(
        hidden,
        whole_ref[:, 2 * width :],
        (((1,), (1,)), ((), ())),
        preferred_element_type=jnp.float32,
    ).astype(jnp.bfloat16)
    own = keep_ref.shape[1]
    core = at_ref[2]
    for p in range(keep_ref.shape[0]):
        start = pl.multiple_of((2 * p + core) * own, own)
        keep_ref[p] = sums_ref[pl.ds(start, own), :]
        start = pl.multiple_of((2 * p + 1 - core) * own, own)
        send_ref[p] = sums_ref[pl.ds(start, own), :]


def body(
    mixer_input,
    time_step,
    damping,
    input_map,
    readout,
    skip_gain,
    out_gain,
    out_weight,
    residual,
    channel_gain,
    value_weight,
    gate_weight,
    value_taps,
    gate_taps,
    down_weight,
):
    half = value_weight.shape[1] // 2
    packed = pl.pallas_call(
        pack_kernel,
        out_shape=jax.ShapeDtypeStruct((4, value_weight.shape[0], 3 * half), jnp.bfloat16),
        in_specs=[VMEM] * 3,
        out_specs=VMEM,
        name="pack",
    )(value_weight, gate_weight, down_weight.T)
    crossed = lax.all_to_all(packed, ("yh", "yl"), 0, 0, tiled=True)
    pieces = z_ring(crossed.reshape(-1, 3 * half))
    pair_resid = pair_rows(residual)
    mixed_y = mixer_branch(
        mixer_input, time_step, damping, input_map, readout, skip_gain, out_gain
    )
    tok_rows = mixer_input.shape[0]
    own_rows, model = residual.shape
    tp_count = lax.axis_size(TP)
    arrived = lax.all_to_all(mixed_y, CHIPS, 0, 0, tiled=True)
    beside = lax.ppermute(arrived, "c", [(0, 1), (1, 0)])
    row_args = (
        jnp.stack([lax.axis_index(a) for a in (*PAIR, "yh")]).astype(jnp.int32),
        arrived,
        beside,
        out_weight,
        channel_gain[None, :],
        *pair_resid,
    )
    state_scratch = [pltpu.VMEM((2 * tok_rows, model), jnp.bfloat16)]
    edge = jax.ShapeDtypeStruct((1, model), jnp.bfloat16)
    near, far = pl.pallas_call(
        edge_kernel,
        out_shape=(edge, edge),
        in_specs=[SMEM] + [VMEM] * 8,
        out_specs=(VMEM, VMEM),
        scratch_shapes=state_scratch,
        name="edge",
compiler_params=pltpu.CompilerParams(vmem_limit_bytes=16 * 2**20),
        cost_estimate=pl.CostEstimate(
            flops=300_000_000, bytes_accessed=6_000_000, transcendentals=0
        ),
    )(*row_args)
    near, far = edges_passed(near, far)
    cells, hidden_state = pl.pallas_call(
        rows_kernel,
        out_shape=(
            jax.ShapeDtypeStruct((2 * tok_rows, model), jnp.bfloat16),
            jax.ShapeDtypeStruct((own_rows, model), jnp.bfloat16),
        ),
        in_specs=[SMEM] + [VMEM] * 8,
        out_specs=(VMEM, VMEM),
        scratch_shapes=state_scratch,
        name="rows",
compiler_params=pltpu.CompilerParams(vmem_limit_bytes=20 * 2**20),
        cost_estimate=pl.CostEstimate(
            flops=1_000_000_000, bytes_accessed=6_000_000, transcendentals=0
        ),
    )(*row_args)
    state_wide = hidden_state.astype(jnp.float32)
    place = jnp.stack([lax.axis_index(a) for a in ("z", "yh", "c")]).astype(jnp.int32)
    shift = lax.axis_index("yl") * half
    taps = [lax.dynamic_slice(t, (0, shift), (3, half)) for t in (value_taps, gate_taps)]
    share = jax.ShapeDtypeStruct((tp_count, own_rows, model), jnp.bfloat16)
    keep, send = pl.pallas_call(
        ffn_kernel,
        out_shape=(share, share),
        in_specs=[SMEM] + [VMEM] * (5 + len(pieces)),
        out_specs=(VMEM, VMEM),
        scratch_shapes=[
            pltpu.VMEM((model, 3 * half), jnp.bfloat16),
            pltpu.VMEM((2 * tok_rows + 16, model), jnp.bfloat16),
            pltpu.VMEM((2 * tok_rows, model), jnp.bfloat16),
        ],
        name="ffn",
compiler_params=pltpu.CompilerParams(vmem_limit_bytes=26 * 2**20),
        cost_estimate=pl.CostEstimate(
            flops=1_300_000_000, bytes_accessed=6_000_000, transcendentals=100_000
        ),
    )(place, cells, near, far, *taps, *pieces)
    other = lax.ppermute(send, "c", [(0, 1), (1, 0)])
    both = (keep.astype(jnp.float32) + other.astype(jnp.float32)).astype(jnp.bfloat16)
    parts = lax.all_to_all(both, CHIPS, 0, 0, tiled=True)
    summed = parts.astype(jnp.float32).sum(axis=0)
    return (state_wide + summed).astype(jnp.bfloat16)


def solution(mesh):
    fine = Mesh(mesh.devices.reshape(8, 2, 2, 4, 2), ("z", "yh", "yl", "x", "c"))
    in_specs = (
        P(SP, TP),
        P(None, TP),
        P(None, SP, TP),
        P(None, None, TP, None, None),
        P(None, None, TP, None, None),
        P(TP),
        P(TP),
        P(),
        P((*SP, *TP), None),
        P(),
        P(SP, TP),
        P(SP, TP),
        P(None, TP),
        P(None, TP),
        P(TP, SP),
    )
    out_specs = P((*SP, *TP), None)

    return jax.shard_map(body, mesh=fine, in_specs=in_specs, out_specs=out_specs, check_vma=False)
```
